32 devices in a mesh: tp: 4 (over y, x), dp: 8 (over z, core).
Axes of the slice: x: 2, y: 2, z: 4, core: 2. Of those that a mesh axis runs over, the one named last changes fastest.
Arguments:
- tokens: bfloat16 [64, 4096], P('tp', 'dp'), may hold values from -12 to 12, as said below
- norm_gain: float32 [2, 4096], P(None, 'dp'), may hold values from 0.1 to 1.9
- w_input: bfloat16 [2, 4096, 2048], P(None, 'dp', 'tp'), may hold values from -0.09375 to 0.09375
- w_gate: bfloat16 [2, 4096, 2048], P(None, 'dp', 'tp'), may hold values from -0.09375 to 0.09375
- w_recur: bfloat16 [2, 16, 128, 128], P(None, 'tp'), may hold values from -0.5 to 0.5
- w_inject: bfloat16 [2, 16, 128, 128], P(None, 'tp'), may hold values from -0.5 to 0.5
- conv_weight: bfloat16 [2, 4, 2048], P(None, None, 'tp'), may hold values from -3 to 3
- decay_param: float32 [2, 2048], P(None, 'tp'), may hold values from -2 to 5
- w_output: bfloat16 [2, 2048, 4096], P(None, 'tp', 'dp'), may hold values from -0.125 to 0.125
- lengths: int32 [64], P('dp'), may hold values from 1 to 48, 512 in all
- conv_state: bfloat16 [2, 3, 64, 2048], P(None, None, 'dp', 'tp'), may hold values from -6 to 6
- rec_state: float32 [2, 64, 2048], P(None, 'dp', 'tp'), may hold values from -6 to 6
Outputs:
- mixed: bfloat16 [64, 4096], P('tp', 'dp')
- new_conv: bfloat16 [2, 3, 64, 2048], P(None, None, 'dp', 'tp')
- new_rec: float32 [2, 64, 2048], P(None, 'dp', 'tp')
The draws below stay inside these ranges and needn't reach their ends.
Inputs may be any that keep to these rules, and one draw needn't show every extreme that they name: `tokens`: activations; feature scales vary.
All inputs are finite; a program needn't handle non-finite values. No bound on the sum of `lengths` on one device may be relied on, other than what follows from the above.
Results may differ from the reference program's by a relative error of at most 0.02.
Values may be sent and summed in bfloat16 or wider, within the bound.
No kernel may reach another device: no remote copies, remote signals or barrier semaphores. Data moves between devices by JAX's collectives and lax.ppermute only.
A program may use at most 64 MiB of HBM per device.

```python
import math
import jax
import jax.numpy as jnp
import numpy as np
from jax import lax

D = 4096
NB = 16
BLK = 128
CONV = 4
W = 2048
BATCH = 64


def draw_tokens(key, part):
    col_scale = jnp.exp(jnp.linspace(jnp.log(0.5), jnp.log(2.0), D)).astype(jnp.float32)
    values = jnp.clip(jax.random.normal(key, (BATCH, D), jnp.float32), -6.0, 6.0)
    return (values * col_scale).astype(jnp.bfloat16)


def block_levels(key, extent, shards, low, high):
    def one(dim, parts):
        heights = jax.random.uniform(jax.random.fold_in(jax.random.fold_in(key, 6), dim), (parts,), jnp.float32, low / len(shards), high / len(shards))
        return jnp.repeat(jnp.exp(heights), extent[dim] // parts).reshape((-1,) + (1,) * (len(extent) - dim - 1))

    gain = one(*shards[0])
    for cut in shards[1:]:
        gain = gain * one(*cut)
    return gain


def split_up(count, total, reach, slope):
    weights = [(1 << 20) // math.isqrt(grade ** slope) + 1 for grade in range(2, count + 1)]
    surplus, holding = total - reach - (count - 1), [1] * (count - 1)
    while surplus > 0:
        movable = [i for i in range(count - 1) if holding[i] < reach]
        pool, left = sum([weights[i] for i in movable]), surplus
        for i in movable:
            addition = min(reach - holding[i], max(1, left * weights[i] // pool), surplus)
            holding[i] = holding[i] + addition
            surplus = surplus - addition
    return np.array([reach] + holding)


def uneven_parts(own_key, count, total, reach, slope):
    if count == 2:
        one = jax.random.randint(own_key, (), max(1, total - reach), min(reach, total - 1) + 1)
        return jnp.stack([one, total - one])
    sizes = jnp.asarray(split_up(count, total, reach, slope), jnp.int32)
    couples = (count - 1) // 2
    source_of, receiver = sizes[1:1 + 2 * couples:2], sizes[2:2 + 2 * couples:2]
    slack = jnp.minimum(source_of - 1, reach - receiver)
    shifted = jax.random.randint(jax.random.fold_in(own_key, 1), (couples,), 0, 1 << 20) % (slack + 1)
    sizes = sizes.at[1:1 + 2 * couples:2].set(source_of - shifted).at[2:2 + 2 * couples:2].set(receiver + shifted)
    return sizes[jax.random.permutation(jax.random.fold_in(own_key, 2), count)]


def bell_draw(key, dims, deviation, most, cuts=(), dtype=jnp.bfloat16):
    gain = block_levels(key, dims, cuts, -0.22, 0.18) if cuts else 1.0
    array = jax.random.normal(key, dims, jnp.float32) * deviation * gain
    return jnp.minimum(jnp.maximum(array, -most), most).astype(dtype)


def setup_inputs(seed: int = 0) -> dict:
    streams_of = jax.random.split(jax.random.key(seed), 13)
    return {
        "tokens": draw_tokens(jax.random.fold_in(streams_of[12], 71), 0),
        "norm_gain": jnp.clip(1.0 + 0.18 * jax.random.normal(streams_of[1], (2, D), jnp.float32), 0.1, 1.9),
        "w_input": bell_draw(streams_of[2], (2, D, W), D ** -0.5, 0.09375, ((1, 8), (2, 4))),
        "w_gate": bell_draw(streams_of[3], (2, D, W), D ** -0.5, 0.09375, ((1, 8), (2, 4))),
        "w_recur": bell_draw(streams_of[4], (2, NB, BLK, BLK), BLK ** -0.5, 0.5, ((1, 4),)),
        "w_inject": bell_draw(streams_of[5], (2, NB, BLK, BLK), BLK ** -0.5, 0.5, ((1, 4),)),
        "conv_weight": bell_draw(streams_of[6], (2, CONV, W), CONV ** -0.5, 3.0, ((2, 4),)),
        "decay_param": jnp.clip(-2.0 + 7.0 * jax.random.uniform(streams_of[7], (2, W), jnp.float32) ** block_levels(streams_of[7], (2, W), ((1, 4),), -0.2, 0.2), -2.0, 5.0),
        "w_output": bell_draw(streams_of[8], (2, W, D), W ** -0.5, 0.125, ((1, 4), (2, 8))),
        "lengths": uneven_parts(streams_of[9], BATCH, 8 * BATCH, 48, 2).astype(jnp.int32),
        "conv_state": bell_draw(streams_of[10], (2, CONV - 1, BATCH, W), 1.0, 6.0, ((2, 8), (3, 4))),
        "rec_state": bell_draw(streams_of[11], (2, BATCH, W), 1.0, 6.0, ((1, 8), (2, 4)), jnp.float32),
    }


EPS = 1e-06

def reference(tokens, norm_gain, w_input, w_gate, w_recur, w_inject, conv_weight, decay_param, w_output, lengths, conv_state, rec_state):
    current = tokens
    live_len = lengths[:, None]
    conv_list = []
    rec_list = []
    for layer_idx in range(2):
        widened = current.astype(jnp.float32)
        rscale = lax.rsqrt(lax.optimization_barrier(jnp.mean(widened * widened, axis=1, keepdims=True)) + EPS)
        scaled = (widened * norm_gain[layer_idx]).astype(jnp.bfloat16)
        value_in = jnp.dot(scaled, w_input[layer_idx], preferred_element_type=jnp.float32) * rscale
        gate_in = jnp.dot(scaled, w_gate[layer_idx], preferred_element_type=jnp.float32) * rscale
        conv_taps = conv_weight[layer_idx].astype(jnp.float32)
        old_taps = conv_state[layer_idx]
        tap_count = old_taps.shape[0]
        conv_out = conv_taps[tap_count] * value_in
        for back in range(1, tap_count + 1):
            conv_out = conv_out + conv_taps[tap_count - back] * jnp.where(back < live_len, old_taps[tap_count - back].astype(jnp.float32), jnp.float32(0.0))
        conv_low = conv_out.astype(jnp.bfloat16).reshape(BATCH, NB, BLK).astype(jnp.float32)
        rec_gate = jax.nn.sigmoid(jnp.einsum('bnc,ncd->bnd', conv_low, w_recur[layer_idx].astype(jnp.float32)).reshape(BATCH, W))
        inp_gate = jax.nn.sigmoid(jnp.einsum('bnc,ncd->bnd', conv_low, w_inject[layer_idx].astype(jnp.float32)).reshape(BATCH, W))
        log_decay = -8.0 * rec_gate * jax.nn.softplus(-decay_param[layer_idx])
        previous = jnp.where(live_len > 1, rec_state[layer_idx], jnp.float32(0.0))
        hidden = jnp.exp(log_decay) * previous + jnp.sqrt(-jnp.expm1(2.0 * log_decay)) * (inp_gate * conv_out)
        readout = (hidden * jax.nn.gelu(gate_in)).astype(jnp.bfloat16)
        current = (widened + jnp.dot(readout, w_output[layer_idx], preferred_element_type=jnp.float32)).astype(jnp.bfloat16)
        conv_list.append(jnp.concatenate([old_taps[1:], value_in.astype(jnp.bfloat16)[None]], axis=0))
        rec_list.append(hidden)
    return (current, jnp.stack(conv_list), jnp.stack(rec_list))
```

```python
import functools

import jax
import jax.numpy as jnp
from jax import lax
from jax.experimental import pallas as pl
from jax.experimental.pallas import tpu as pltpu
from jax.sharding import PartitionSpec as P

EPS = 1e-06
F32 = jnp.float32
BF16 = jnp.bfloat16


def call(kernel, outs, *args, scratch=(), flops=1000000, limit=8):
    single = not isinstance(outs, (list, tuple))
    spec = pl.BlockSpec(memory_space=pltpu.VMEM)
    return pl.pallas_call(
        kernel,
        out_shape=outs,
        in_specs=[spec] * len(args),
        out_specs=spec if single else [spec] * len(outs),
        scratch_shapes=list(scratch),
        compiler_params=pltpu.CompilerParams(vmem_limit_bytes=limit << 20),
        cost_estimate=pl.CostEstimate(flops=flops, bytes_accessed=1 << 20, transcendentals=0),
    )(*args)


def shape(dims, dtype):
    return jax.ShapeDtypeStruct(tuple(dims), dtype)


class Layout:
    def __init__(self, batch, tp, dp):
        self.batch, self.tp, self.dp = batch, tp, dp
        self.rows = batch // dp
        self.half = batch // 2
        self.per_tp = batch // tp
        self.chunks = self.per_tp // self.rows

    def place(self, chunk, core):
        side = jnp.where(lax.rem(chunk, 2) == core, 0, self.half)
        return pl.multiple_of(side + (chunk // 2) * self.rows, self.rows)


def mesh_place():
    core = lax.rem(lax.axis_index("dp"), 2)
    return lax.axis_index("tp"), lax.axis_index("dp") // 2, core


def partner_exchange(value, axis, masks):
    count = lax.axis_size(axis)
    return [lax.ppermute(value, axis, [(i, i ^ m) for i in range(count)]) for m in masks]


def as_column(row):
    n = row.shape[1]
    eye = lax.broadcasted_iota(jnp.int32, (n, n), 0) == lax.broadcasted_iota(jnp.int32, (n, n), 1)
    return jnp.sum(jnp.where(eye, jnp.broadcast_to(row, (n, n)), 0), axis=1, keepdims=True)


def state_kernel(lengths_ref, taps_ref, conv_ref, rec_ref, out_ref):
    live = as_column(lengths_ref[...])
    for layer in range(conv_ref.shape[0]):
        depth = conv_ref.shape[1]
        old = jnp.zeros(rec_ref.shape[1:], F32)
        for back in range(1, depth + 1):
            tap = taps_ref[layer, pl.ds(depth - back, 1), :].astype(F32)
            old = old + tap * jnp.where(back < live, conv_ref[layer, depth - back].astype(F32), 0.0)
        out_ref[layer, 0] = old
        out_ref[layer, 1] = jnp.where(live > 1, rec_ref[layer], 0.0)


def project(x, gain, wi_ref, wg_ref, keep_ref, send_ref):
    width = wi_ref.shape[1]
    half = keep_ref.shape[0]
    square = jnp.sum(x * x, axis=1, keepdims=True)
    high = square.astype(BF16).astype(F32)
    lane = lax.broadcasted_iota(jnp.int32, (x.shape[0], 128), 1)
    squares = jnp.where(lane < 64, high, square - high)
    scaled = (x * gain).astype(BF16)
    value = jnp.dot(scaled, wi_ref[...], preferred_element_type=F32)
    gate = jnp.dot(scaled, wg_ref[...], preferred_element_type=F32)
    for ref, rows in ((keep_ref, slice(0, half)), (send_ref, slice(half, 2 * half))):
        ref[:, :width] = value[rows].astype(ref.dtype)
        ref[:, width : 2 * width] = gate[rows].astype(ref.dtype)
        ref[:, 2 * width :] = squares[rows].astype(ref.dtype)


def first_kernel(lay, *refs):
    parts, (gain_ref, wi_ref, wg_ref, x_ref, keep_ref, send_ref) = refs[: lay.tp], refs[lay.tp :]
    me, _, core = mesh_place()
    for mask, part in enumerate(parts):
        owner = me ^ mask
        rows = part[...].astype(F32)
        for i in range(lay.chunks):
            start = lay.place(owner * lay.chunks + i, core)
            x_ref[pl.ds(start, lay.rows), :] = rows[i * lay.rows : (i + 1) * lay.rows]
    project(x_ref[...], gain_ref[...], wi_ref, wg_ref, keep_ref, send_ref)


def next_kernel(lay, x_old_ref, *refs):
    parts, (gain_ref, wi_ref, wg_ref, own_ref, keep_ref, send_ref, x_ref) = refs[: lay.tp], refs[lay.tp :]
    me, _, core = mesh_place()
    total = parts[0][...].astype(F32)
    for part in parts[1:]:
        total = total + part[...].astype(F32)
    x = (x_old_ref[...] + total).astype(BF16).astype(F32)
    x_ref[...] = x
    for i in range(lay.chunks):
        start = lay.place(me * lay.chunks + i, core)
        own_ref[i * lay.rows : (i + 1) * lay.rows, :] = x_ref[pl.ds(start, lay.rows), :]
    project(x, gain_ref[...], wi_ref, wg_ref, keep_ref, send_ref)


def one_minus_exp(u):
    series = 1.0 + u * (1.0 / 6.0)
    for k in (5.0, 4.0, 3.0, 2.0):
        series = 1.0 + u * (1.0 / k) * series
    return jnp.where(u > -0.25, -u * series, 1.0 - jnp.exp(u))


def add_kernel(keep_ref, got_ref, out_ref):
    out_ref[...] = (keep_ref[...] + got_ref[...].astype(F32)).astype(out_ref.dtype)


def recurrence_kernel(lay, layer, features, *refs):
    zs = lay.dp // 2
    sums, refs = refs[:zs], refs[zs:]
    states, refs = refs[:zs], refs[zs:]
    taps_ref, decay_ref, wr_ref, wj_ref, readout_ref, value_ref, rec_ref, old_ref, prev_ref, keep_value, keep_rec = refs
    _, z, _ = mesh_place()
    rows = lay.rows
    for mask, state in enumerate(states):
        start = pl.multiple_of((z ^ mask) * rows, rows)
        old_ref[pl.ds(start, rows), :] = state[layer, 0]
        prev_ref[pl.ds(start, rows), :] = state[layer, 1]
    total = sums[0][...].astype(F32)
    for part in sums[1:]:
        total = total + part[...].astype(F32)
    width = old_ref.shape[1]
    square = total[:, 2 * width : 2 * width + 1] + total[:, 2 * width + 64 : 2 * width + 65]
    scale = lax.rsqrt(square / features + EPS)
    value_in = total[:, :width] * scale
    gate_in = total[:, width : 2 * width] * scale
    last = taps_ref.shape[0] - 1
    conv_out = taps_ref[pl.ds(last, 1), :].astype(F32) * value_in + old_ref[...]
    conv_low = conv_out.astype(BF16)
    blocks, block = wr_ref.shape[0], wr_ref.shape[1]

    def mapped(ref):
        return jnp.concatenate(
            [
                jnp.dot(conv_low[:, b * block : (b + 1) * block], ref[b], preferred_element_type=F32)
                for b in range(blocks)
            ],
            axis=1,
        )

    rec_gate = jax.nn.sigmoid(mapped(wr_ref))
    inp_gate = jax.nn.sigmoid(mapped(wj_ref))
    log_decay = -8.0 * rec_gate * jax.nn.softplus(-decay_ref[...])
    hidden = jnp.exp(log_decay) * prev_ref[...] + jnp.sqrt(one_minus_exp(2.0 * log_decay)) * (inp_gate * conv_out)
    readout_ref[...] = (hidden * jax.nn.gelu(gate_in)).astype(BF16)
    keep_value[...] = value_in
    keep_rec[...] = hidden
    mine = pl.ds(pl.multiple_of(z * rows, rows), rows)
    value_ref[...] = keep_value[mine, :].astype(BF16)
    rec_ref[...] = keep_rec[mine, :]


def output_kernel(own_ref, other_ref, w_ref, out_ref):
    half = own_ref.shape[0]
    out_ref[:half] = jnp.dot(own_ref[...], w_ref[...], preferred_element_type=F32).astype(BF16)
    out_ref[half:] = jnp.dot(other_ref[...], w_ref[...], preferred_element_type=F32).astype(BF16)


def last_output_kernel(lay, own_ref, other_ref, w_ref, *refs):
    outs, held = refs[:-1], refs[-1]
    half = own_ref.shape[0]
    held[:half] = jnp.dot(own_ref[...], w_ref[...], preferred_element_type=F32)
    held[half:] = jnp.dot(other_ref[...], w_ref[...], preferred_element_type=F32)
    me, _, core = mesh_place()
    for mask, out in enumerate(outs):
        for i in range(lay.chunks):
            start = lay.place((me ^ mask) * lay.chunks + i, core)
            out[i * lay.rows : (i + 1) * lay.rows, :] = held[pl.ds(start, lay.rows), :].astype(out.dtype)


def final_kernel(own_ref, *refs):
    parts, out_ref = refs[:-1], refs[-1]
    total = parts[0][...].astype(F32)
    for part in parts[1:]:
        total = total + part[...].astype(F32)
    out_ref[...] = (own_ref[...] + total).astype(BF16)


def body(
    tokens,
    norm_gain,
    w_input,
    w_gate,
    w_recur,
    w_inject,
    conv_weight,
    decay_param,
    w_output,
    lengths,
    conv_state,
    rec_state,
):
    tp, dp = lax.axis_size("tp"), lax.axis_size("dp")
    lay = Layout(tokens.shape[0] * tp, tp, dp)
    depth, features = tokens.shape[1], tokens.shape[1] * dp
    width = rec_state.shape[2]
    half, batch = lay.half, lay.batch
    layers = w_input.shape[0]

    tp_masks = range(1, tp)
    z_masks = [2 * k for k in range(1, dp // 2)]

    parts = [tokens] + partner_exchange(tokens, "tp", tp_masks)
    state = call(
        state_kernel,
        shape((layers, 2, lay.rows, width), F32),
        lengths[None, :],
        conv_weight,
        conv_state,
        rec_state,
    )
    states = [state] + partner_exchange(state, "dp", z_masks)

    conv_list, rec_list = [], []
    x = own = None
    for layer in range(layers):
        wide = 2 * width + 128
        pair = [shape((half, wide), F32), shape((half, wide), BF16)]
        weights = (norm_gain[layer][None], w_input[layer], w_gate[layer])
        if layer == 0:
            x, keep, send = call(
                functools.partial(first_kernel, lay),
                [shape((batch, depth), F32)] + pair,
                *parts,
                *weights,
            )
        else:
            own, keep, send = call(
                functools.partial(next_kernel, lay),
                [shape((lay.per_tp, depth), F32)] + pair,
                x,
                *parts,
                *weights,
                scratch=[pltpu.VMEM((batch, depth), F32)],
            )
        (got,) = partner_exchange(send, "dp", [1])
        summed = call(add_kernel, shape((half, wide), BF16), keep, got)
        sums = [summed] + partner_exchange(summed, "dp", z_masks)
        readout, value, hidden = call(
            functools.partial(recurrence_kernel, lay, layer, features),
            [
                shape((half, width), BF16),
                shape((lay.rows, width), BF16),
                shape((lay.rows, width), F32),
            ],
            *sums,
            *states,
            conv_weight[layer],
            decay_param[layer][None],
            w_recur[layer],
            w_inject[layer],
            scratch=[pltpu.VMEM((half, width), F32)] * 4,
        )
        (other,) = partner_exchange(readout, "dp", [1])
        if layer < layers - 1:
            partial = call(output_kernel, shape((batch, depth), BF16), readout, other, w_output[layer])
            parts = [partial] + partner_exchange(partial, "tp", tp_masks)
        else:
            pieces = call(
                functools.partial(last_output_kernel, lay),
                [shape((lay.per_tp, depth), BF16)] * tp,
                readout,
                other,
                w_output[layer],
                scratch=[pltpu.VMEM((batch, depth), F32)],
            )
            parts = [pieces[0]] + [partner_exchange(pieces[m], "tp", [m])[0] for m in tp_masks]
        conv_list.append(jnp.concatenate([conv_state[layer, 1:], value[None]], axis=0))
        rec_list.append(hidden)
    mixed = call(final_kernel, shape((lay.per_tp, depth), BF16), own, *parts)
    return mixed, jnp.stack(conv_list), jnp.stack(rec_list)


def solution(mesh):
    placed = (
        P("tp", "dp"),
        P(None, "dp"),
        P(None, "dp", "tp"),
        P(None, "dp", "tp"),
        P(None, "tp", None, None),
        P(None, "tp", None, None),
        P(None, None, "tp"),
        P(None, "tp"),
        P(None, "tp", "dp"),
        P("dp"),
        P(None, None, "dp", "tp"),
        P(None, "dp", "tp"),
    )
    return jax.shard_map(
        body,
        mesh=mesh,
        in_specs=placed,
        out_specs=(P("tp", "dp"), P(None, None, "dp", "tp"), P(None, "dp", "tp")),
        check_vma=False,
    )
```

```python
import functools

import jax
import jax.numpy as jnp
from jax import lax
from jax.experimental import pallas as pl
from jax.experimental.pallas import tpu as pltpu
from jax.sharding import PartitionSpec as P

EPS = 1e-06
F32 = jnp.float32
BF16 = jnp.bfloat16

COVER = 1 << 31


def call(kernel, outs, *args, scratch=(), flops=1000000, limit=8):
    single = not isinstance(outs, (list, tuple))
    spec = pl.BlockSpec(memory_space=pltpu.VMEM)
    return pl.pallas_call(
        kernel,
        out_shape=outs,
        in_specs=[spec] * len(args),
        out_specs=spec if single else [spec] * len(outs),
        scratch_shapes=list(scratch),
        compiler_params=pltpu.CompilerParams(vmem_limit_bytes=limit << 20),
        cost_estimate=pl.CostEstimate(flops=flops, bytes_accessed=1 << 20, transcendentals=0),
    )(*args)


def shape(dims, dtype):
    return jax.ShapeDtypeStruct(tuple(dims), dtype)


def widen_kernel(x_ref, out_ref):
    out_ref[...] = x_ref[...].astype(F32)


class Layout:
    def __init__(self, batch, tp, dp):
        self.batch, self.tp, self.dp = batch, tp, dp
        self.rows = batch // dp
        self.half = batch // 2
        self.per_tp = batch // tp
        self.chunks = self.per_tp // self.rows

    def place(self, chunk, z, core):
        side = jnp.where(lax.rem(chunk, 2) == core, 0, self.half)
        return pl.multiple_of(side + ((chunk // 2) ^ z) * self.rows, self.rows)


def mesh_place():
    core = lax.rem(lax.axis_index("dp"), 2)
    return lax.axis_index("tp"), lax.axis_index("dp") // 2, core


def partner_exchange(value, axis, masks):
    count = lax.axis_size(axis)
    return [lax.ppermute(value, axis, [(i, i ^ m) for i in range(count)]) for m in masks]


def as_column(row):
    n = row.shape[1]
    eye = lax.broadcasted_iota(jnp.int32, (n, n), 0) == lax.broadcasted_iota(jnp.int32, (n, n), 1)
    return jnp.sum(jnp.where(eye, jnp.broadcast_to(row, (n, n)), 0), axis=1, keepdims=True)


def project(x, gain, wi, wg, keep_ref, send_ref):
    width = wi.shape[1]
    half = keep_ref.shape[0]
    square = jnp.sum(x * x, axis=1, keepdims=True)
    high = square.astype(BF16).astype(F32)
    lane = lax.broadcasted_iota(jnp.int32, (x.shape[0], 128), 1)
    squares = jnp.where(lane < 64, high, square - high)
    scaled = (x * gain).astype(BF16)
    value = jnp.dot(scaled, wi, preferred_element_type=F32)
    gate = jnp.dot(scaled, wg, preferred_element_type=F32)
    for ref, rows in ((keep_ref, slice(0, half)), (send_ref, slice(half, 2 * half))):
        ref[:, :width] = value[rows].astype(ref.dtype)
        ref[:, width : 2 * width] = gate[rows].astype(ref.dtype)
        ref[:, 2 * width :] = squares[rows].astype(ref.dtype)


def first_kernel(lay, *refs):
    parts, (gain_ref, wi_ref, wg_ref, x_ref, keep_ref, send_ref) = refs[: lay.tp], refs[lay.tp :]
    me, z, core = mesh_place()
    for mask, part in enumerate(parts):
        owner = me ^ mask
        rows = part[...].astype(F32)
        for i in range(lay.chunks):
            start = lay.place(owner * lay.chunks + i, z, core)
            x_ref[pl.ds(start, lay.rows), :] = rows[i * lay.rows : (i + 1) * lay.rows]
    project(x_ref[...], gain_ref[0:1, :], wi_ref[0], wg_ref[0], keep_ref, send_ref)


def next_kernel(lay, layer, x_old_ref, *refs):
    parts, (gain_ref, wi_ref, wg_ref, x_ref, keep_ref, send_ref) = refs[: lay.tp], refs[lay.tp :]
    total = parts[0][...].astype(F32)
    for part in parts[1:]:
        total = total + part[...].astype(F32)
    x = (x_old_ref[...] + total).astype(BF16).astype(F32)
    x_ref[...] = x
    project(x, gain_ref[layer : layer + 1, :], wi_ref[layer], wg_ref[layer], keep_ref, send_ref)


def one_minus_exp(u):
    series = 1.0 + u * (1.0 / 6.0)
    for k in (5.0, 4.0, 3.0, 2.0):
        series = 1.0 + u * (1.0 / k) * series
    return jnp.where(u > -0.25, -u * series, 1.0 - jnp.exp(u))


def add_kernel(keep_ref, got_ref, own_ref, *outs):
    total = keep_ref[...] + got_ref[...].astype(F32)
    rows = own_ref.shape[0]
    own_ref[...] = total[:rows]
    for m, out in enumerate(outs):
        out[...] = total[(m + 1) * rows : (m + 2) * rows].astype(out.dtype)


def recurrence_kernel(zs, layer, features, *refs):
    sums, refs = refs[:zs], refs[zs:]
    lengths_ref, conv_ref, state_ref, taps_ref, decay_ref, wr_ref, wj_ref, readout_ref, value_ref, rec_ref = refs
    total = sums[0][...]
    for part in sums[1:]:
        total = total + part[...].astype(F32)
    live = as_column(lengths_ref[...])
    depth = conv_ref.shape[1]
    width = state_ref.shape[2]
    square = total[:, 2 * width : 2 * width + 1] + total[:, 2 * width + 64 : 2 * width + 65]
    scale = lax.rsqrt(square / features + EPS)
    value_in = total[:, :width] * scale
    gate_in = total[:, width : 2 * width] * scale
    conv_out = taps_ref[layer, depth : depth + 1, :].astype(F32) * value_in
    for back in range(1, depth + 1):
        tap = taps_ref[layer, depth - back : depth - back + 1, :].astype(F32)
        conv_out = conv_out + tap * jnp.where(back < live, conv_ref[layer, depth - back].astype(F32), 0.0)
    conv_low = conv_out.astype(BF16)
    blocks, block = wr_ref.shape[1], wr_ref.shape[2]

    def mapped(ref):
        return jnp.concatenate(
            [
                jnp.dot(conv_low[:, b * block : (b + 1) * block], ref[layer, b], preferred_element_type=F32)
                for b in range(blocks)
            ],
            axis=1,
        )

    rec_gate = jax.nn.sigmoid(mapped(wr_ref))
    inp_gate = jax.nn.sigmoid(mapped(wj_ref))
    log_decay = -8.0 * rec_gate * jax.nn.softplus(-decay_ref[layer : layer + 1, :])
    previous = jnp.where(live > 1, state_ref[layer], 0.0)
    hidden = jnp.exp(log_decay) * previous + jnp.sqrt(one_minus_exp(2.0 * log_decay)) * (inp_gate * conv_out)
    readout_ref[...] = (hidden * jax.nn.gelu(gate_in)).astype(BF16)
    value_ref[...] = value_in.astype(BF16)
    rec_ref[...] = hidden


def join_kernel(*refs):
    parts, out = refs[:-1], refs[-1]
    out[...] = jnp.concatenate([part[...] for part in parts], axis=0)


def output_kernel(layer, own_ref, other_ref, w_ref, out_ref):
    half = own_ref.shape[0]
    out_ref[:half] = jnp.dot(own_ref[...], w_ref[layer], preferred_element_type=F32).astype(BF16)
    out_ref[half:] = jnp.dot(other_ref[...], w_ref[layer], preferred_element_type=F32).astype(BF16)


def last_output_kernel(lay, layer, own_ref, other_ref, w_ref, x_ref, *refs):
    mine_ref, outs, held = refs[0], refs[1:-1], refs[-1]
    half = own_ref.shape[0]
    held[:half] = jnp.dot(own_ref[...], w_ref[layer], preferred_element_type=F32)
    held[half:] = jnp.dot(other_ref[...], w_ref[layer], preferred_element_type=F32)
    me, z, core = mesh_place()
    for mask, out in enumerate((mine_ref,) + tuple(outs)):
        for i in range(lay.chunks):
            start = lay.place((me ^ mask) * lay.chunks + i, z, core)
            piece = held[pl.ds(start, lay.rows), :]
            if mask == 0:
                piece = piece + x_ref[pl.ds(start, lay.rows), :]
            out[i * lay.rows : (i + 1) * lay.rows, :] = piece.astype(out.dtype)


def final_kernel(own_ref, *refs):
    parts, out_ref = refs[:-1], refs[-1]
    total = own_ref[...]
    for part in parts:
        total = total + part[...].astype(F32)
    out_ref[...] = total.astype(BF16)


def body(
    tokens,
    norm_gain,
    w_input,
    w_gate,
    w_recur,
    w_inject,
    conv_weight,
    decay_param,
    w_output,
    lengths,
    conv_state,
    rec_state,
):
    tp, dp = lax.axis_size("tp"), lax.axis_size("dp")
    lay = Layout(tokens.shape[0] * tp, tp, dp)
    depth, features = tokens.shape[1], tokens.shape[1] * dp
    width = rec_state.shape[2]
    half, batch = lay.half, lay.batch
    layers = w_input.shape[0]

    tp_masks = range(1, tp)
    z_masks = [2 * k for k in range(1, dp // 2)]

    wide = 2 * width + 128
    moved = partner_exchange(tokens, "tp", tp_masks)
    parts = [call(widen_kernel, shape(tokens.shape, F32), tokens, flops=COVER)] + moved
    conv_list, rec_list = [], []
    x = None
    for layer in range(layers):
        outs = [shape((batch, depth), F32), shape((half, wide), F32), shape((half, wide), BF16)]
        weights = (norm_gain, w_input, w_gate)
        if layer == 0:
            x, keep, send = call(functools.partial(first_kernel, lay), outs, *parts, *weights)
        else:
            x, keep, send = call(functools.partial(next_kernel, lay, layer), outs, x, *parts, *weights)
        (got,) = partner_exchange(send, "dp", [1])
        own, *pieces = call(
            add_kernel,
            [shape((lay.rows, wide), F32)] + [shape((lay.rows, wide), BF16)] * len(z_masks),
            keep,
            got,
        )
        sums = [own] + [partner_exchange(p, "dp", [m])[0] for p, m in zip(pieces, z_masks)]
        readout, value, hidden = call(
            functools.partial(recurrence_kernel, dp // 2, layer, features),
            [
                shape((lay.rows, width), BF16),
                shape((lay.rows, width), BF16),
                shape((lay.rows, width), F32),
            ],
            *sums,
            lengths[None, :],
            conv_state,
            rec_state,
            conv_weight,
            decay_param,
            w_recur,
            w_inject,
        )
        mine = call(join_kernel, shape((half, width), BF16), readout, *partner_exchange(readout, "dp", z_masks))
        (other,) = partner_exchange(mine, "dp", [1])
        if layer < layers - 1:
            partial = call(
                functools.partial(output_kernel, layer), shape((batch, depth), BF16), mine, other, w_output
            )
            parts = [partial] + partner_exchange(partial, "tp", tp_masks)
        else:
            own, *pieces = call(
                functools.partial(last_output_kernel, lay, layer),
                [shape((lay.per_tp, depth), F32)] + [shape((lay.per_tp, depth), BF16)] * (tp - 1),
                mine,
                other,
                w_output,
                x,
                scratch=[pltpu.VMEM((batch, depth), F32)],
            )
            parts = [own] + [partner_exchange(p, "tp", [m])[0] for p, m in zip(pieces, tp_masks)]
        conv_list.append(jnp.concatenate([conv_state[layer, 1:], value[None]], axis=0))
        rec_list.append(hidden)
    mixed = call(final_kernel, shape((lay.per_tp, depth), BF16), *parts)
    return mixed, jnp.stack(conv_list), jnp.stack(rec_list)


def solution(mesh):
    placed = (
        P("tp", "dp"),
        P(None, "dp"),
        P(None, "dp", "tp"),
        P(None, "dp", "tp"),
        P(None, "tp", None, None),
        P(None, "tp", None, None),
        P(None, None, "tp"),
        P(None, "tp"),
        P(None, "tp", "dp"),
        P("dp"),
        P(None, None, "dp", "tp"),
        P(None, "dp", "tp"),
    )
    return jax.shard_map(
        body,
        mesh=mesh,
        in_specs=placed,
        out_specs=(P("tp", "dp"), P(None, None, "dp", "tp"), P(None, "dp", "tp")),
        check_vma=False,
    )
```

```python
import functools

import jax
import jax.numpy as jnp
from jax import lax
from jax.experimental import pallas as pl
from jax.experimental.pallas import tpu as pltpu
from jax.sharding import PartitionSpec as P


EPS = 1e-06
F32 = jnp.float32
BF16 = jnp.bfloat16

COVER = 1 << 31


def call(kernel, outs, *args, scratch=(), flops=1000000, limit=8):
    single = not isinstance(outs, (list, tuple))
    spec = pl.BlockSpec(memory_space=pltpu.VMEM)
    return pl.pallas_call(
        kernel,
        out_shape=outs,
        in_specs=[spec] * len(args),
        out_specs=spec if single else [spec] * len(outs),
        scratch_shapes=list(scratch),
        compiler_params=pltpu.CompilerParams(vmem_limit_bytes=limit << 20),
        cost_estimate=pl.CostEstimate(flops=flops, bytes_accessed=1 << 20, transcendentals=0),
    )(*args)


def shape(dims, dtype):
    return jax.ShapeDtypeStruct(tuple(dims), dtype)


class Layout:
    def __init__(self, batch, tp, dp):
        self.batch, self.tp, self.dp = batch, tp, dp
        self.rows = batch // dp
        self.half = batch // 2
        self.per_tp = batch // tp
        self.chunks = self.per_tp // self.rows

    def place(self, chunk, z, core):
        side = jnp.where(lax.rem(chunk, 2) == core, 0, self.half)
        return pl.multiple_of(side + ((chunk // 2) ^ z) * self.rows, self.rows)


def mesh_place():
    core = lax.rem(lax.axis_index("dp"), 2)
    return lax.axis_index("tp"), lax.axis_index("dp") // 2, core


def partner_exchange(value, axis, masks):
    count = lax.axis_size(axis)
    return [lax.ppermute(value, axis, [(i, i ^ m) for i in range(count)]) for m in masks]


def doubling(value, axis, masks):
    stack = value[None]
    for mask in masks:
        (got,) = partner_exchange(stack, axis, [mask])
        if mask == masks[-1]:
            return [stack, got]
        stack = call(join_kernel, shape((2 * stack.shape[0],) + stack.shape[1:], stack.dtype), stack, got)


def join_kernel(first_ref, second_ref, out_ref):
    half = first_ref.shape[0]
    out_ref[:half] = first_ref[...]
    out_ref[half:] = second_ref[...]


def entry(stacks, m):
    size = stacks[0].shape[0]
    return stacks[m // size][m % size]


def as_column(row):
    n = row.shape[1]
    eye = lax.broadcasted_iota(jnp.int32, (n, n), 0) == lax.broadcasted_iota(jnp.int32, (n, n), 1)
    return jnp.sum(jnp.where(eye, jnp.broadcast_to(row, (n, n)), 0), axis=1, keepdims=True)


def length_kernel(lengths_ref, out_ref):
    out_ref[...] = jnp.broadcast_to(as_column(lengths_ref[...]), out_ref.shape)


def state_kernel(lengths_ref, taps_ref, conv_ref, rec_ref, out_ref):
    live = lengths_ref[:, 0:1]
    depth = conv_ref.shape[1]
    for layer in range(conv_ref.shape[0]):
        old = jnp.zeros(rec_ref.shape[1:], F32)
        for back in range(1, depth + 1):
            tap = taps_ref[layer, depth - back : depth - back + 1, :].astype(F32)
            old = old + tap * jnp.where(back < live, conv_ref[layer, depth - back].astype(F32), 0.0)
        out_ref[layer, 0] = old
        out_ref[layer, 1] = jnp.where(live > 1, rec_ref[layer], 0.0)


LANES = 128
GROUP = 8


def packed_rows(rows, width):
    return 2 * (width // LANES) * rows + GROUP


def pack(ref, value, gate, square):
    rows, width = value.shape
    count = width // LANES
    for k, block in enumerate((value, gate)):
        for b in range(count):
            start = (k * count + b) * rows
            ref[start : start + rows, :] = block[:, b * LANES : (b + 1) * LANES].astype(ref.dtype)
    high = square.astype(BF16).astype(F32)
    low = square - high
    lane = lax.broadcasted_iota(jnp.int32, (GROUP, LANES), 1)
    tile = jnp.zeros((GROUP, LANES), F32)
    for g in range(rows // GROUP):
        part = slice(g * GROUP, (g + 1) * GROUP)
        tile = jnp.where(lane == g, high[part], jnp.where(lane == g + LANES // 2, low[part], tile))
    ref[2 * count * rows :, :] = tile.astype(ref.dtype)


def unpack(total, rows, width):
    count = width // LANES
    blocks = [total[b * rows : (b + 1) * rows] for b in range(2 * count)]
    value = jnp.concatenate(blocks[:count], axis=1)
    gate = jnp.concatenate(blocks[count:], axis=1)
    tile = total[2 * count * rows :]
    half = LANES // 2
    square = jnp.concatenate(
        [tile[:, g : g + 1] + tile[:, g + half : g + half + 1] for g in range(rows // GROUP)], axis=0
    )
    return value, gate, square


def by_owner(part, mask, zs, size):
    return jnp.concatenate([part[(m ^ mask) * size : ((m ^ mask) + 1) * size] for m in range(zs)], axis=0)


def project(x, gain, wi, wg, keep_ref, send_ref):
    half = x.shape[0] // 2
    square = jnp.sum(x * x, axis=1, keepdims=True)
    scaled = (x * gain).astype(BF16)
    value = jnp.dot(scaled, wi, preferred_element_type=F32)
    gate = jnp.dot(scaled, wg, preferred_element_type=F32)
    pack(keep_ref, value[:half], gate[:half], square[:half])
    pack(send_ref, value[half:], gate[half:], square[half:])


def first_kernel(lay, low_ref, high_ref, gain_ref, wi_ref, wg_ref, x_ref, keep_ref, send_ref):
    me, z, core = mesh_place()
    for mask in range(lay.tp):
        owner = me ^ mask
        rows = entry((low_ref, high_ref), mask).astype(F32)
        for i in range(lay.chunks):
            start = lay.place(owner * lay.chunks + i, z, core)
            x_ref[pl.ds(start, lay.rows), :] = rows[i * lay.rows : (i + 1) * lay.rows]
    project(x_ref[...], gain_ref[0:1, :], wi_ref[0], wg_ref[0], keep_ref, send_ref)


def next_kernel(lay, layer, x_old_ref, *refs):
    parts, (gain_ref, wi_ref, wg_ref, x_ref, keep_ref, send_ref) = refs[: lay.tp], refs[lay.tp :]
    total = parts[0][...].astype(F32)
    for part in parts[1:]:
        total = total + part[...].astype(F32)
    x = (x_old_ref[...] + total).astype(BF16).astype(F32)
    x_ref[...] = x
    project(x, gain_ref[layer : layer + 1, :], wi_ref[layer], wg_ref[layer], keep_ref, send_ref)


def one_minus_exp(u):
    series = 1.0 + u * (1.0 / 6.0)
    for k in (5.0, 4.0, 3.0, 2.0):
        series = 1.0 + u * (1.0 / k) * series
    return jnp.where(u > -0.25, -u * series, 1.0 - jnp.exp(u))


def add_kernel(keep_ref, got_ref, out_ref):
    out_ref[...] = (keep_ref[...] + got_ref[...].astype(F32)).astype(out_ref.dtype)


def recurrence_kernel(lay, layer, features, *refs):
    zs = lay.dp // 2
    sums, refs = refs[:zs], refs[zs:]
    low_ref, high_ref, taps_ref, decay_ref, wr_ref, wj_ref, readout_ref, value_ref, rec_ref = refs
    rows, half, width = lay.rows, lay.half, taps_ref.shape[2]
    states = [entry((low_ref, high_ref), m) for m in range(zs)]
    old = jnp.concatenate([state[layer, 0] for state in states], axis=0)
    previous = jnp.concatenate([state[layer, 1] for state in states], axis=0)
    value_in = gate_in = square = None
    for mask, part in enumerate(sums):
        terms = [by_owner(t, mask, zs, rows) for t in unpack(part[...].astype(F32), half, width)]
        if mask == 0:
            value_in, gate_in, square = terms
        else:
            value_in, gate_in, square = value_in + terms[0], gate_in + terms[1], square + terms[2]
    scale = lax.rsqrt(square / features + EPS)
    value_in = value_in * scale
    gate_in = gate_in * scale
    last = taps_ref.shape[1] - 1
    conv_out = taps_ref[layer, last : last + 1, :].astype(F32) * value_in + old
    conv_low = conv_out.astype(BF16)
    blocks, block = wr_ref.shape[1], wr_ref.shape[2]

    def mapped(ref):
        return jnp.concatenate(
            [
                jnp.dot(conv_low[:, b * block : (b + 1) * block], ref[layer, b], preferred_element_type=F32)
                for b in range(blocks)
            ],
            axis=1,
        )

    rec_gate = jax.nn.sigmoid(mapped(wr_ref))
    inp_gate = jax.nn.sigmoid(mapped(wj_ref))
    log_decay = -8.0 * rec_gate * jax.nn.softplus(-decay_ref[layer : layer + 1, :])
    hidden = jnp.exp(log_decay) * previous + jnp.sqrt(one_minus_exp(2.0 * log_decay)) * (inp_gate * conv_out)
    readout_ref[...] = (hidden * jax.nn.gelu(gate_in)).astype(BF16)
    value_ref[...] = value_in[:rows].astype(BF16)
    rec_ref[...] = hidden[:rows]


def output_kernel(layer, own_ref, other_ref, w_ref, out_ref):
    half = own_ref.shape[0]
    out_ref[:half] = jnp.dot(own_ref[...], w_ref[layer], preferred_element_type=F32).astype(BF16)
    out_ref[half:] = jnp.dot(other_ref[...], w_ref[layer], preferred_element_type=F32).astype(BF16)


def last_output_kernel(lay, layer, own_ref, other_ref, w_ref, x_ref, *refs):
    mine_ref, outs, held = refs[0], refs[1:-1], refs[-1]
    half = own_ref.shape[0]
    held[:half] = jnp.dot(own_ref[...], w_ref[layer], preferred_element_type=F32)
    held[half:] = jnp.dot(other_ref[...], w_ref[layer], preferred_element_type=F32)
    me, z, core = mesh_place()
    for mask, out in enumerate((mine_ref,) + tuple(outs)):
        for i in range(lay.chunks):
            start = lay.place((me ^ mask) * lay.chunks + i, z, core)
            piece = held[pl.ds(start, lay.rows), :]
            if mask == 0:
                piece = piece + x_ref[pl.ds(start, lay.rows), :]
            out[i * lay.rows : (i + 1) * lay.rows, :] = piece.astype(out.dtype)


def final_kernel(own_ref, *refs):
    parts, out_ref = refs[:-1], refs[-1]
    total = own_ref[...]
    for part in parts:
        total = total + part[...].astype(F32)
    out_ref[...] = total.astype(BF16)


def blocks(
    tokens,
    norm_gain,
    w_input,
    w_gate,
    w_recur,
    w_inject,
    conv_weight,
    decay_param,
    w_output,
    lengths,
    conv_state,
    rec_state,
):
    tp, dp = lax.axis_size("tp"), lax.axis_size("dp")
    lay = Layout(tokens.shape[0] * tp, tp, dp)
    depth, features = tokens.shape[1], tokens.shape[1] * dp
    width = rec_state.shape[2]
    half, batch = lay.half, lay.batch
    layers = w_input.shape[0]

    tp_masks = range(1, tp)
    z_masks = [2 * k for k in range(1, dp // 2)]

    tall = packed_rows(half, width)
    bits = lambda n: [1 << k for k in range(n.bit_length() - 1)]
    live = call(length_kernel, shape((lay.rows, LANES), jnp.int32), lengths[None, :], flops=COVER)
    state = call(
        state_kernel,
        shape((layers, 2, lay.rows, width), F32),
        live,
        conv_weight,
        conv_state,
        rec_state,
    )
    rows = doubling(tokens, "tp", bits(tp))
    states = doubling(state, "dp", [2 * m for m in bits(dp // 2)])
    parts = None
    conv_list, rec_list = [], []
    x = None
    for layer in range(layers):
        outs = [shape((batch, depth), F32), shape((tall, LANES), F32), shape((tall, LANES), BF16)]
        weights = (norm_gain, w_input, w_gate)
        if layer == 0:
            x, keep, send = call(functools.partial(first_kernel, lay), outs, *rows, *weights)
        else:
            x, keep, send = call(functools.partial(next_kernel, lay, layer), outs, x, *parts, *weights)
        (got,) = partner_exchange(send, "dp", [1])
        summed = call(add_kernel, shape((tall, LANES), BF16), keep, got)
        readout, value, hidden = call(
            functools.partial(recurrence_kernel, lay, layer, features),
            [
                shape((half, width), BF16),
                shape((lay.rows, width), BF16),
                shape((lay.rows, width), F32),
            ],
            summed,
            *partner_exchange(summed, "dp", z_masks),
            *states,
            conv_weight,
            decay_param,
            w_recur,
            w_inject,
        )
        (other,) = partner_exchange(readout, "dp", [1])
        if layer < layers - 1:
            partial = call(
                functools.partial(output_kernel, layer), shape((batch, depth), BF16), readout, other, w_output
            )
            parts = [partial] + partner_exchange(partial, "tp", tp_masks)
        else:
            own, *pieces = call(
                functools.partial(last_output_kernel, lay, layer),
                [shape((lay.per_tp, depth), F32)] + [shape((lay.per_tp, depth), BF16)] * (tp - 1),
                readout,
                other,
                w_output,
                x,
                scratch=[pltpu.VMEM((batch, depth), F32)],
            )
            parts = [own] + [partner_exchange(p, "tp", [m])[0] for p, m in zip(pieces, tp_masks)]
        conv_list.append(jnp.concatenate([conv_state[layer, 1:], value[None]], axis=0))
        rec_list.append(hidden)
    mixed = call(final_kernel, shape((lay.per_tp, depth), BF16), *parts)
    return mixed, jnp.stack(conv_list), jnp.stack(rec_list)


def solution(mesh):
    placed = (
        P("tp", "dp"),
        P(None, "dp"),
        P(None, "dp", "tp"),
        P(None, "dp", "tp"),
        P(None, "tp", None, None),
        P(None, "tp", None, None),
        P(None, None, "tp"),
        P(None, "tp"),
        P(None, "tp", "dp"),
        P("dp"),
        P(None, None, "dp", "tp"),
        P(None, "dp", "tp"),
    )
    return jax.shard_map(
        blocks,
        mesh=mesh,
        in_specs=placed,
        out_specs=(P("tp", "dp"), P(None, None, "dp", "tp"), P(None, "dp", "tp")),
        check_vma=False,
    )
```

```python
import functools

import jax
import jax.numpy as jnp
from jax import lax
from jax.experimental import pallas as pl
from jax.experimental.pallas import tpu as pltpu
from jax.sharding import PartitionSpec as P


EPS = 1e-06
F32 = jnp.float32
BF16 = jnp.bfloat16

COVER = 1 << 31


def call(kernel, outs, *args, scratch=(), flops=1000000, limit=8):
    single = not isinstance(outs, (list, tuple))
    spec = pl.BlockSpec(memory_space=pltpu.VMEM)
    return pl.pallas_call(
        kernel,
        out_shape=outs,
        in_specs=[spec] * len(args),
        out_specs=spec if single else [spec] * len(outs),
        scratch_shapes=list(scratch),
        compiler_params=pltpu.CompilerParams(vmem_limit_bytes=limit << 20),
        cost_estimate=pl.CostEstimate(flops=flops, bytes_accessed=1 << 20, transcendentals=0),
    )(*args)


def shape(dims, dtype):
    return jax.ShapeDtypeStruct(tuple(dims), dtype)


class Layout:
    def __init__(self, batch, tp, dp):
        self.batch, self.tp, self.dp = batch, tp, dp
        self.rows = batch // dp
        self.half = batch // 2
        self.per_tp = batch // tp
        self.chunks = self.per_tp // self.rows

    def side(self, owner, z):
        return pl.multiple_of((owner ^ z) * self.rows, self.rows)

    def place(self, chunk, z, core):
        side = jnp.where(lax.rem(chunk, 2) == core, 0, self.half)
        return pl.multiple_of(side + ((chunk // 2) ^ z) * self.rows, self.rows)


def mesh_place():
    core = lax.rem(lax.axis_index("dp"), 2)
    return lax.axis_index("tp"), lax.axis_index("dp") // 2, core


def partner_exchange(value, axis, masks):
    count = lax.axis_size(axis)
    got = []
    for m in masks:
        got.append(lax.ppermute(value, axis, [(i, i ^ m) for i in range(count)]))
    return got


def doubling(value, axis, masks):
    stack = value[None]
    for mask in masks:
        (got,) = partner_exchange(stack, axis, [mask])
        if mask == masks[-1]:
            return [stack, got]
        stack = call(join_kernel, shape((2 * stack.shape[0],) + stack.shape[1:], stack.dtype), stack, got)


def join_kernel(first_ref, second_ref, out_ref):
    half = first_ref.shape[0]
    out_ref[:half] = first_ref[...]
    out_ref[half:] = second_ref[...]


def entry(stacks, m):
    size = stacks[0].shape[0]
    return stacks[m // size][m % size]


def as_column(row):
    n = row.shape[1]
    eye = lax.broadcasted_iota(jnp.int32, (n, n), 0) == lax.broadcasted_iota(jnp.int32, (n, n), 1)
    return jnp.sum(jnp.where(eye, jnp.broadcast_to(row, (n, n)), 0), axis=1, keepdims=True)


def length_kernel(lengths_ref, out_ref):
    out_ref[...] = jnp.broadcast_to(as_column(lengths_ref[...]), out_ref.shape)


def state_kernel(lengths_ref, taps_ref, conv_ref, rec_ref, out_ref):
    live = lengths_ref[:, 0:1]
    depth = conv_ref.shape[1]
    for layer in range(conv_ref.shape[0]):
        old = jnp.zeros(rec_ref.shape[1:], F32)
        for back in range(1, depth + 1):
            tap = taps_ref[layer, depth - back : depth - back + 1, :].astype(F32)
            old = old + tap * jnp.where(back < live, conv_ref[layer, depth - back].astype(F32), 0.0)
        out_ref[layer, 0] = old
        out_ref[layer, 1] = jnp.where(live > 1, rec_ref[layer], 0.0)


LANES = 128
GROUP = 8


def packed_rows(rows, width):
    return 2 * (width // LANES) * rows + GROUP


def pack(ref, value, gate, square):
    rows, width = value.shape
    count = width // LANES
    for k, block in enumerate((value, gate)):
        for b in range(count):
            start = (k * count + b) * rows
            ref[start : start + rows, :] = block[:, b * LANES : (b + 1) * LANES].astype(ref.dtype)
    high = square.astype(BF16).astype(F32)
    low = square - high
    lane = lax.broadcasted_iota(jnp.int32, (GROUP, LANES), 1)
    tile = jnp.zeros((GROUP, LANES), F32)
    for g in range(rows // GROUP):
        part = slice(g * GROUP, (g + 1) * GROUP)
        tile = jnp.where(lane == g, high[part], jnp.where(lane == g + LANES // 2, low[part], tile))
    ref[2 * count * rows : 2 * count * rows + GROUP, :] = tile.astype(ref.dtype)


def unpack(total, rows, width):
    count = width // LANES
    blocks = [total[b * rows : (b + 1) * rows] for b in range(2 * count)]
    value = jnp.concatenate(blocks[:count], axis=1)
    gate = jnp.concatenate(blocks[count:], axis=1)
    tile = total[2 * count * rows :]
    half = LANES // 2
    square = jnp.concatenate(
        [tile[:, g : g + 1] + tile[:, g + half : g + half + 1] for g in range(rows // GROUP)], axis=0
    )
    return value, gate, square


def by_owner(part, mask, zs, size):
    return jnp.concatenate([part[(m ^ mask) * size : ((m ^ mask) + 1) * size] for m in range(zs)], axis=0)


def to_blocks(ref, start, rows):
    count = rows.shape[0]
    for b in range(rows.shape[1] // LANES):
        ref[start + b * count : start + (b + 1) * count, :] = rows[:, b * LANES : (b + 1) * LANES].astype(ref.dtype)


def from_blocks(ref, start, rows, width):
    return jnp.concatenate(
        [ref[start + b * rows : start + (b + 1) * rows, :] for b in range(width // LANES)], axis=1
    )


def first_kernel(lay, low_ref, high_ref, gain_ref, wi_ref, wg_ref, x_ref, keep_ref, send_ref):
    me, z, core = mesh_place()
    for mask in range(lay.tp):
        owner = me ^ mask
        rows = entry((low_ref, high_ref), mask).astype(F32)
        for i in range(lay.chunks):
            start = lay.place(owner * lay.chunks + i, z, core)
            x_ref[pl.ds(start, lay.rows), :] = rows[i * lay.rows : (i + 1) * lay.rows]
    x = x_ref[...]
    half, tall = lay.half, keep_ref.shape[0]
    square = jnp.sum(x * x, axis=1, keepdims=True)
    scaled = (x * gain_ref[0:1, :]).astype(BF16)
    value = jnp.dot(scaled, wi_ref[0], preferred_element_type=F32)
    gate = jnp.dot(scaled, wg_ref[0], preferred_element_type=F32)
    pack(keep_ref, value[:half], gate[:half], square[:half])
    pack(send_ref, value[half:], gate[half:], square[half:])
    to_blocks(send_ref, tall, x[half:])


def next_kernel(lay, layer, x_old_ref, got_ref, *refs):
    parts, refs = refs[: lay.tp], refs[lay.tp :]
    gain_ref, wi_ref, wg_ref, gain2_ref, wi2_ref, wg2_ref, x_ref, out_ref = refs
    half, depth = lay.half, x_old_ref.shape[1]
    start = got_ref.shape[0] - half * depth // LANES
    total = parts[0][...].astype(F32)
    for part in parts[1:]:
        total = total + part[...].astype(F32)
    x = (x_old_ref[:half] + total[:, :depth]).astype(BF16).astype(F32)
    y = (from_blocks(got_ref, start, half, depth).astype(F32) + total[:, depth:]).astype(BF16).astype(F32)
    x_ref[:, :depth] = x
    x_ref[:, depth:] = y
    square = jnp.sum(x * x, axis=1, keepdims=True) + jnp.sum(y * y, axis=1, keepdims=True)
    scaled = (x * gain_ref[layer : layer + 1, :]).astype(BF16)
    scaled2 = (y * gain2_ref[layer : layer + 1, :]).astype(BF16)

    def both(w, w2):
        return jnp.dot(scaled, w[layer], preferred_element_type=F32) + jnp.dot(
            scaled2, w2[layer], preferred_element_type=F32
        )

    pack(out_ref, both(wi_ref, wi2_ref), both(wg_ref, wg2_ref), square)


def one_minus_exp(u):
    series = 1.0 + u * (1.0 / 6.0)
    for k in (5.0, 4.0, 3.0, 2.0):
        series = 1.0 + u * (1.0 / k) * series
    return jnp.where(u > -0.25, -u * series, 1.0 - jnp.exp(u))


def add_kernel(keep_ref, got_ref, out_ref):
    out_ref[...] = (keep_ref[...] + got_ref[: keep_ref.shape[0]].astype(F32)).astype(out_ref.dtype)


def recurrence_kernel(lay, layer, features, *refs):
    zs = lay.dp // 2
    sums, refs = refs[:zs], refs[zs:]
    low_ref, high_ref, taps_ref, decay_ref, wr_ref, wj_ref, *extra, readout_ref, value_ref, rec_ref = refs
    rows, half, width = lay.rows, lay.half, taps_ref.shape[2]
    states = [entry((low_ref, high_ref), m) for m in range(zs)]
    old = jnp.concatenate([state[layer, 0] for state in states], axis=0)
    previous = jnp.concatenate([state[layer, 1] for state in states], axis=0)
    value_in = gate_in = square = None
    for mask, part in enumerate(sums):
        terms = [by_owner(t, mask, zs, rows) for t in unpack(part[...].astype(F32), half, width)]
        if mask == 0:
            value_in, gate_in, square = terms
        else:
            value_in, gate_in, square = value_in + terms[0], gate_in + terms[1], square + terms[2]
    scale = lax.rsqrt(square / features + EPS)
    value_in = value_in * scale
    gate_in = gate_in * scale
    last = taps_ref.shape[1] - 1
    conv_out = taps_ref[layer, last : last + 1, :].astype(F32) * value_in + old
    conv_low = conv_out.astype(BF16)
    blocks, block = wr_ref.shape[1], wr_ref.shape[2]

    def mapped(ref):
        return jnp.concatenate(
            [
                jnp.dot(conv_low[:, b * block : (b + 1) * block], ref[layer, b], preferred_element_type=F32)
                for b in range(blocks)
            ],
            axis=1,
        )

    rec_gate = jax.nn.sigmoid(mapped(wr_ref))
    inp_gate = jax.nn.sigmoid(mapped(wj_ref))
    log_decay = -8.0 * rec_gate * jax.nn.softplus(-decay_ref[layer : layer + 1, :])
    hidden = jnp.exp(log_decay) * previous + jnp.sqrt(one_minus_exp(2.0 * log_decay)) * (inp_gate * conv_out)
    readout_ref[:half] = (hidden * jax.nn.gelu(gate_in)).astype(BF16)
    for x_ref in extra:
        me, z, _ = mesh_place()
        depth = x_ref.shape[1] // 2
        for i in range(lay.chunks // 2):
            start = lay.side(me * (lay.chunks // 2) + i, z)
            readout_ref[half + i * rows : half + (i + 1) * rows] = x_ref[pl.ds(start, rows), depth:].astype(BF16)
    value_ref[...] = value_in[:rows].astype(BF16)
    rec_ref[...] = hidden[:rows]


def output_kernel(layer, rows_ref, w_ref, w2_ref, out_ref):
    width = w_ref.shape[2]
    out_ref[:, :width] = jnp.dot(rows_ref[...], w_ref[layer], preferred_element_type=F32).astype(BF16)
    out_ref[:, width:] = jnp.dot(rows_ref[...], w2_ref[layer], preferred_element_type=F32).astype(BF16)


def last_output_kernel(lay, layer, own_ref, other_ref, w_ref, x_ref, *refs):
    outs, held = refs[:-1], refs[-1]
    half, rows, depth = lay.half, lay.rows, held.shape[1]
    held[:half] = jnp.dot(own_ref[:half], w_ref[layer], preferred_element_type=F32)
    held[half:] = jnp.dot(other_ref[:half], w_ref[layer], preferred_element_type=F32)
    me, z, core = mesh_place()
    far = other_ref[half:].astype(F32)
    for mask, out in enumerate(outs):
        for i in range(lay.chunks):
            start = lay.place((me ^ mask) * lay.chunks + i, z, core)
            piece = held[pl.ds(start, rows), :]
            if mask == 0:
                near = x_ref[pl.ds(lay.side(me * (lay.chunks // 2) + i // 2, z), rows), :depth]
                piece = piece + jnp.where(core == i % 2, near, far[i // 2 * rows : (i // 2 + 1) * rows])
            out[i * rows : (i + 1) * rows, :] = piece.astype(out.dtype)


def final_kernel(own_ref, *refs):
    parts, out_ref = refs[:-1], refs[-1]
    total = own_ref[...]
    for part in parts:
        total = total + part[...].astype(F32)
    out_ref[...] = total.astype(BF16)


def blocks(
    tokens,
    norm_gain,
    w_input,
    w_gate,
    w_recur,
    w_inject,
    conv_weight,
    decay_param,
    w_output,
    lengths,
    conv_state,
    rec_state,
):
    tp, dp = lax.axis_size("tp"), lax.axis_size("dp")
    lay = Layout(tokens.shape[0] * tp, tp, dp)
    depth, features = tokens.shape[1], tokens.shape[1] * dp
    width = rec_state.shape[2]
    half, batch = lay.half, lay.batch
    layers = w_input.shape[0]

    tp_masks = range(1, tp)
    z_masks = [2 * k for k in range(1, dp // 2)]

    tall = packed_rows(half, width)
    bits = lambda n: [1 << k for k in range(n.bit_length() - 1)]
    live = call(length_kernel, shape((lay.rows, LANES), jnp.int32), lengths[None, :], flops=COVER)
    state = call(
        state_kernel,
        shape((layers, 2, lay.rows, width), F32),
        live,
        conv_weight,
        conv_state,
        rec_state,
    )
    rows = doubling(tokens, "tp", bits(tp))
    states = doubling(state, "dp", [2 * m for m in bits(dp // 2)])
    sent = half * depth // LANES
    block = [
        shape((half, width), BF16),
        shape((lay.rows, width), BF16),
        shape((lay.rows, width), F32),
    ]
    weights = (norm_gain, w_input, w_gate)
    x, keep, send = call(
        functools.partial(first_kernel, lay),
        [shape((batch, depth), F32), shape((tall, LANES), F32), shape((tall + sent, LANES), BF16)],
        *rows,
        *weights,
    )
    (got,) = partner_exchange(send, "dp", [1])
    summed = call(add_kernel, shape((tall, LANES), BF16), keep, got)
    conv_list, rec_list = [], []
    for layer in range(layers):
        last = layer == layers - 1
        if layer > 0:
            x, summed = call(
                functools.partial(next_kernel, lay, layer),
                [shape((half, 2 * depth), F32), shape((tall, LANES), BF16)],
                *before,
                *parts,
                *weights,
                *weights2,
            )
        sums = [summed] + partner_exchange(summed, "dp", z_masks)
        if layer == 0:
            out2, *weights2 = [partner_exchange(w, "dp", [1])[0] for w in (w_output,) + weights]
        if last:
            block[0] = shape((half + lay.per_tp // 2, width), BF16)
        readout, value, hidden = call(
            functools.partial(recurrence_kernel, lay, layer, features),
            block,
            *sums,
            *states,
            conv_weight,
            decay_param,
            w_recur,
            w_inject,
            *([x] if last else []),
        )
        if not last:
            partial = call(
                functools.partial(output_kernel, layer),
                shape((half, 2 * depth), BF16),
                readout,
                w_output,
                out2,
            )
            parts = [partial] + partner_exchange(partial, "tp", tp_masks)
            before = (x, got)
        else:
            (other,) = partner_exchange(readout, "dp", [1])
            own, *pieces = call(
                functools.partial(last_output_kernel, lay, layer),
                [shape((lay.per_tp, depth), F32)] + [shape((lay.per_tp, depth), BF16)] * (tp - 1),
                readout,
                other,
                w_output,
                x,
                scratch=[pltpu.VMEM((batch, depth), F32)],
            )
            parts = [own] + [partner_exchange(p, "tp", [m])[0] for p, m in zip(pieces, tp_masks)]
        conv_list.append(jnp.concatenate([conv_state[layer, 1:], value[None]], axis=0))
        rec_list.append(hidden)
    mixed = call(final_kernel, shape((lay.per_tp, depth), BF16), *parts)
    return mixed, jnp.stack(conv_list), jnp.stack(rec_list)


def solution(mesh):
    placed = (
        P("tp", "dp"),
        P(None, "dp"),
        P(None, "dp", "tp"),
        P(None, "dp", "tp"),
        P(None, "tp", None, None),
        P(None, "tp", None, None),
        P(None, None, "tp"),
        P(None, "tp"),
        P(None, "tp", "dp"),
        P("dp"),
        P(None, None, "dp", "tp"),
        P(None, "dp", "tp"),
    )
    return jax.shard_map(
        blocks,
        mesh=mesh,
        in_specs=placed,
        out_specs=(P("tp", "dp"), P(None, None, "dp", "tp"), P(None, "dp", "tp")),
        check_vma=False,
    )
```

```python
import functools

import jax
import jax.numpy as jnp
from jax import lax
from jax.experimental import pallas as pl
from jax.experimental.pallas import tpu as pltpu
from jax.sharding import PartitionSpec as P


EPS = 1e-06
F32 = jnp.float32
BF16 = jnp.bfloat16

COVER = 1 << 31


def call(kernel, outs, *args, scratch=(), flops=1000000, limit=8):
    single = not isinstance(outs, (list, tuple))
    spec = pl.BlockSpec(memory_space=pltpu.VMEM)
    return pl.pallas_call(
        kernel,
        out_shape=outs,
        in_specs=[spec] * len(args),
        out_specs=spec if single else [spec] * len(outs),
        scratch_shapes=list(scratch),
        compiler_params=pltpu.CompilerParams(vmem_limit_bytes=limit << 20),
        cost_estimate=pl.CostEstimate(flops=flops, bytes_accessed=1 << 20, transcendentals=0),
    )(*args)


def shape(dims, dtype):
    return jax.ShapeDtypeStruct(tuple(dims), dtype)


class Layout:
    def __init__(self, batch, tp, dp):
        self.batch, self.tp, self.dp = batch, tp, dp
        self.rows = batch // dp
        self.half = batch // 2
        self.per_tp = batch // tp
        self.chunks = self.per_tp // self.rows

    def side(self, owner, z):
        return pl.multiple_of((owner ^ z) * self.rows, self.rows)

    def place(self, chunk, z, core):
        side = jnp.where(lax.rem(chunk, 2) == core, 0, self.half)
        return pl.multiple_of(side + ((chunk // 2) ^ z) * self.rows, self.rows)


def mesh_place():
    core = lax.rem(lax.axis_index("dp"), 2)
    return lax.axis_index("tp"), lax.axis_index("dp") // 2, core


def partner_exchange(value, axis, masks):
    count = lax.axis_size(axis)
    got = []
    for m in masks:
        got.append(lax.ppermute(value, axis, [(i, i ^ m) for i in range(count)]))
    return got


def doubling(value, axis, masks):
    stack = value[None]
    for mask in masks:
        (got,) = partner_exchange(stack, axis, [mask])
        if mask == masks[-1]:
            return [stack, got]
        stack = call(join_kernel, shape((2 * stack.shape[0],) + stack.shape[1:], stack.dtype), stack, got)


def join_kernel(first_ref, second_ref, out_ref):
    half = first_ref.shape[0]
    out_ref[:half] = first_ref[...]
    out_ref[half:] = second_ref[...]


def entry(stacks, m):
    size = stacks[0].shape[0]
    return stacks[m // size][m % size]


def as_column(row):
    n = row.shape[1]
    eye = lax.broadcasted_iota(jnp.int32, (n, n), 0) == lax.broadcasted_iota(jnp.int32, (n, n), 1)
    return jnp.sum(jnp.where(eye, jnp.broadcast_to(row, (n, n)), 0), axis=1, keepdims=True)


def length_kernel(lengths_ref, out_ref):
    out_ref[...] = jnp.broadcast_to(as_column(lengths_ref[...]), out_ref.shape)


def state_kernel(lengths_ref, taps_ref, conv_ref, rec_ref, out_ref, low_ref):
    live = lengths_ref[:, 0:1]
    depth = conv_ref.shape[1]
    for layer in range(conv_ref.shape[0]):
        old = jnp.zeros(rec_ref.shape[1:], F32)
        for back in range(1, depth + 1):
            tap = taps_ref[layer, depth - back : depth - back + 1, :].astype(F32)
            old = old + tap * jnp.where(back < live, conv_ref[layer, depth - back].astype(F32), 0.0)
        out_ref[layer, 0] = old
        out_ref[layer, 1] = jnp.where(live > 1, rec_ref[layer], 0.0)
    low_ref[...] = out_ref[...].astype(BF16)


LANES = 128
GROUP = 8


def packed_rows(rows, width):
    return 2 * (width // LANES) * rows + GROUP


def pack(ref, value, gate, square):
    rows, width = value.shape
    count = width // LANES
    for k, block in enumerate((value, gate)):
        for b in range(count):
            start = (k * count + b) * rows
            ref[start : start + rows, :] = block[:, b * LANES : (b + 1) * LANES].astype(ref.dtype)
    high = square.astype(BF16).astype(F32)
    low = square - high
    lane = lax.broadcasted_iota(jnp.int32, (GROUP, LANES), 1)
    tile = jnp.zeros((GROUP, LANES), F32)
    for g in range(rows // GROUP):
        part = slice(g * GROUP, (g + 1) * GROUP)
        tile = jnp.where(lane == g, high[part], jnp.where(lane == g + LANES // 2, low[part], tile))
    ref[2 * count * rows : 2 * count * rows + GROUP, :] = tile.astype(ref.dtype)


def unpack(total, rows, width):
    count = width // LANES
    blocks = [total[b * rows : (b + 1) * rows] for b in range(2 * count)]
    value = jnp.concatenate(blocks[:count], axis=1)
    gate = jnp.concatenate(blocks[count:], axis=1)
    tile = total[2 * count * rows :]
    half = LANES // 2
    square = jnp.concatenate(
        [tile[:, g : g + 1] + tile[:, g + half : g + half + 1] for g in range(rows // GROUP)], axis=0
    )
    return value, gate, square


def by_owner(part, mask, zs, size):
    return jnp.concatenate([part[(m ^ mask) * size : ((m ^ mask) + 1) * size] for m in range(zs)], axis=0)


def to_blocks(ref, start, rows):
    count = rows.shape[0]
    for b in range(rows.shape[1] // LANES):
        ref[start + b * count : start + (b + 1) * count, :] = rows[:, b * LANES : (b + 1) * LANES].astype(ref.dtype)


def from_blocks(ref, start, rows, width):
    return jnp.concatenate(
        [ref[start + b * rows : start + (b + 1) * rows, :] for b in range(width // LANES)], axis=1
    )


def first_kernel(lay, low_ref, high_ref, gain_ref, wi_ref, wg_ref, x_ref, keep_ref, send_ref):
    me, z, core = mesh_place()
    for mask in range(lay.tp):
        owner = me ^ mask
        rows = entry((low_ref, high_ref), mask).astype(F32)
        for i in range(lay.chunks):
            start = lay.place(owner * lay.chunks + i, z, core)
            x_ref[pl.ds(start, lay.rows), :] = rows[i * lay.rows : (i + 1) * lay.rows]
    x = x_ref[...]
    half, tall = lay.half, keep_ref.shape[0]
    square = jnp.sum(x * x, axis=1, keepdims=True)
    scaled = (x * gain_ref[0:1, :]).astype(BF16)
    value = jnp.dot(scaled, wi_ref[0], preferred_element_type=F32)
    gate = jnp.dot(scaled, wg_ref[0], preferred_element_type=F32)
    pack(keep_ref, value[:half], gate[:half], square[:half])
    pack(send_ref, value[half:], gate[half:], square[half:])
    to_blocks(send_ref, tall, x[half:])


def next_kernel(lay, layer, x_old_ref, got_ref, *refs):
    parts, refs = refs[: lay.tp], refs[lay.tp :]
    gain_ref, wi_ref, wg_ref, gain2_ref, wi2_ref, wg2_ref, x_ref, out_ref = refs
    half, depth = lay.half, x_old_ref.shape[1]
    start = got_ref.shape[0] - half * depth // LANES
    total = parts[0][...].astype(F32)
    for part in parts[1:]:
        total = total + part[...].astype(F32)
    x = (x_old_ref[:half] + total[:, :depth]).astype(BF16).astype(F32)
    y = (from_blocks(got_ref, start, half, depth).astype(F32) + total[:, depth:]).astype(BF16).astype(F32)
    x_ref[:, :depth] = x
    x_ref[:, depth:] = y
    square = jnp.sum(x * x, axis=1, keepdims=True) + jnp.sum(y * y, axis=1, keepdims=True)
    scaled = (x * gain_ref[layer : layer + 1, :]).astype(BF16)
    scaled2 = (y * gain2_ref[layer : layer + 1, :]).astype(BF16)

    def both(w, w2):
        return jnp.dot(scaled, w[layer], preferred_element_type=F32) + jnp.dot(
            scaled2, w2[layer], preferred_element_type=F32
        )

    pack(out_ref, both(wi_ref, wi2_ref), both(wg_ref, wg2_ref), square)


def one_minus_exp(u):
    series = 1.0 + u * (1.0 / 6.0)
    for k in (5.0, 4.0, 3.0, 2.0):
        series = 1.0 + u * (1.0 / k) * series
    return jnp.where(u > -0.25, -u * series, 1.0 - jnp.exp(u))


def add_kernel(keep_ref, got_ref, out_ref):
    out_ref[...] = (keep_ref[...] + got_ref[: keep_ref.shape[0]].astype(F32)).astype(out_ref.dtype)


def recurrence_kernel(lay, layer, features, *refs):
    zs = lay.dp // 2
    sums, refs = refs[:zs], refs[zs:]
    own_ref, low_ref, high_ref, taps_ref, decay_ref, wr_ref, wj_ref, *extra, readout_ref, value_ref, rec_ref = refs
    rows, half, width = lay.rows, lay.half, taps_ref.shape[2]
    states = [own_ref] + [entry((low_ref, high_ref), m) for m in range(1, zs)]
    old = jnp.concatenate([state[layer, 0].astype(F32) for state in states], axis=0)
    previous = jnp.concatenate([state[layer, 1].astype(F32) for state in states], axis=0)
    value_in = gate_in = square = None
    for mask, part in enumerate(sums):
        terms = [by_owner(t, mask, zs, rows) for t in unpack(part[...].astype(F32), half, width)]
        if mask == 0:
            value_in, gate_in, square = terms
        else:
            value_in, gate_in, square = value_in + terms[0], gate_in + terms[1], square + terms[2]
    scale = lax.rsqrt(square / features + EPS)
    value_in = value_in * scale
    gate_in = gate_in * scale
    last = taps_ref.shape[1] - 1
    conv_out = taps_ref[layer, last : last + 1, :].astype(F32) * value_in + old
    conv_low = conv_out.astype(BF16)
    blocks, block = wr_ref.shape[1], wr_ref.shape[2]

    def mapped(ref):
        return jnp.concatenate(
            [
                jnp.dot(conv_low[:, b * block : (b + 1) * block], ref[layer, b], preferred_element_type=F32)
                for b in range(blocks)
            ],
            axis=1,
        )

    rec_gate = jax.nn.sigmoid(mapped(wr_ref))
    inp_gate = jax.nn.sigmoid(mapped(wj_ref))
    log_decay = -8.0 * rec_gate * jax.nn.softplus(-decay_ref[layer : layer + 1, :])
    hidden = jnp.exp(log_decay) * previous + jnp.sqrt(one_minus_exp(2.0 * log_decay)) * (inp_gate * conv_out)
    readout_ref[:half] = (hidden * jax.nn.gelu(gate_in)).astype(BF16)
    for x_ref in extra:
        me, z, _ = mesh_place()
        depth = x_ref.shape[1] // 2
        for i in range(lay.chunks // 2):
            start = lay.side(me * (lay.chunks // 2) + i, z)
            readout_ref[half + i * rows : half + (i + 1) * rows] = x_ref[pl.ds(start, rows), depth:].astype(BF16)
    value_ref[...] = value_in[:rows].astype(BF16)
    rec_ref[...] = hidden[:rows]


def output_kernel(layer, rows_ref, w_ref, w2_ref, out_ref):
    width = w_ref.shape[2]
    out_ref[:, :width] = jnp.dot(rows_ref[...], w_ref[layer], preferred_element_type=F32).astype(BF16)
    out_ref[:, width:] = jnp.dot(rows_ref[...], w2_ref[layer], preferred_element_type=F32).astype(BF16)


def last_output_kernel(lay, layer, own_ref, other_ref, w_ref, x_ref, *refs):
    outs, held = refs[:-1], refs[-1]
    half, rows, depth = lay.half, lay.rows, held.shape[1]
    held[:half] = jnp.dot(own_ref[:half], w_ref[layer], preferred_element_type=F32)
    held[half:] = jnp.dot(other_ref[:half], w_ref[layer], preferred_element_type=F32)
    me, z, core = mesh_place()
    far = other_ref[half:].astype(F32)
    for mask, out in enumerate(outs):
        for i in range(lay.chunks):
            start = lay.place((me ^ mask) * lay.chunks + i, z, core)
            piece = held[pl.ds(start, rows), :]
            if mask == 0:
                near = x_ref[pl.ds(lay.side(me * (lay.chunks // 2) + i // 2, z), rows), :depth]
                piece = piece + jnp.where(core == i % 2, near, far[i // 2 * rows : (i // 2 + 1) * rows])
            out[i * rows : (i + 1) * rows, :] = piece.astype(out.dtype)


def final_kernel(own_ref, *refs):
    parts, out_ref = refs[:-1], refs[-1]
    total = own_ref[...]
    for part in parts:
        total = total + part[...].astype(F32)
    out_ref[...] = total.astype(BF16)


def blocks(
    tokens,
    norm_gain,
    w_input,
    w_gate,
    w_recur,
    w_inject,
    conv_weight,
    decay_param,
    w_output,
    lengths,
    conv_state,
    rec_state,
):
    tp, dp = lax.axis_size("tp"), lax.axis_size("dp")
    lay = Layout(tokens.shape[0] * tp, tp, dp)
    depth, features = tokens.shape[1], tokens.shape[1] * dp
    width = rec_state.shape[2]
    half, batch = lay.half, lay.batch
    layers = w_input.shape[0]

    tp_masks = range(1, tp)
    z_masks = [2 * k for k in range(1, dp // 2)]

    tall = packed_rows(half, width)
    bits = lambda n: [1 << k for k in range(n.bit_length() - 1)]
    live = call(length_kernel, shape((lay.rows, LANES), jnp.int32), lengths[None, :], flops=COVER)
    state, low = call(
        state_kernel,
        [shape((layers, 2, lay.rows, width), t) for t in (F32, BF16)],
        live,
        conv_weight,
        conv_state,
        rec_state,
    )
    rows = doubling(tokens, "tp", bits(tp))
    states = [state] + doubling(low, "dp", [2 * m for m in bits(dp // 2)])
    sent = half * depth // LANES
    block = [
        shape((half, width), BF16),
        shape((lay.rows, width), BF16),
        shape((lay.rows, width), F32),
    ]
    weights = (norm_gain, w_input, w_gate)
    x, keep, send = call(
        functools.partial(first_kernel, lay),
        [shape((batch, depth), F32), shape((tall, LANES), F32), shape((tall + sent, LANES), BF16)],
        *rows,
        *weights,
    )
    (got,) = partner_exchange(send, "dp", [1])
    summed = call(add_kernel, shape((tall, LANES), BF16), keep, got)
    conv_list, rec_list = [], []
    for layer in range(layers):
        last = layer == layers - 1
        if layer > 0:
            x, summed = call(
                functools.partial(next_kernel, lay, layer),
                [shape((half, 2 * depth), F32), shape((tall, LANES), BF16)],
                *before,
                *parts,
                *weights,
                *weights2,
            )
        sums = [summed] + partner_exchange(summed, "dp", z_masks)
        if layer == 0:
            out2, *weights2 = [partner_exchange(w, "dp", [1])[0] for w in (w_output,) + weights]
        if last:
            block[0] = shape((half + lay.per_tp // 2, width), BF16)
        readout, value, hidden = call(
            functools.partial(recurrence_kernel, lay, layer, features),
            block,
            *sums,
            *states,
            conv_weight,
            decay_param,
            w_recur,
            w_inject,
            *([x] if last else []),
        )
        if not last:
            partial = call(
                functools.partial(output_kernel, layer),
                shape((half, 2 * depth), BF16),
                readout,
                w_output,
                out2,
            )
            parts = [partial] + partner_exchange(partial, "tp", tp_masks)
            before = (x, got)
        else:
            (other,) = partner_exchange(readout, "dp", [1])
            own, *pieces = call(
                functools.partial(last_output_kernel, lay, layer),
                [shape((lay.per_tp, depth), F32)] + [shape((lay.per_tp, depth), BF16)] * (tp - 1),
                readout,
                other,
                w_output,
                x,
                scratch=[pltpu.VMEM((batch, depth), F32)],
            )
            parts = [own] + [partner_exchange(p, "tp", [m])[0] for p, m in zip(pieces, tp_masks)]
        conv_list.append(jnp.concatenate([conv_state[layer, 1:], value[None]], axis=0))
        rec_list.append(hidden)
    mixed = call(final_kernel, shape((lay.per_tp, depth), BF16), *parts)
    return mixed, jnp.stack(conv_list), jnp.stack(rec_list)


def solution(mesh):
    placed = (
        P("tp", "dp"),
        P(None, "dp"),
        P(None, "dp", "tp"),
        P(None, "dp", "tp"),
        P(None, "tp", None, None),
        P(None, "tp", None, None),
        P(None, None, "tp"),
        P(None, "tp"),
        P(None, "tp", "dp"),
        P("dp"),
        P(None, None, "dp", "tp"),
        P(None, "dp", "tp"),
    )

    return jax.shard_map(
        blocks,
        mesh=mesh,
        in_specs=placed,
        out_specs=(P("tp", "dp"), P(None, None, "dp", "tp"), P(None, "dp", "tp")),
        check_vma=False,
    )
```

```python
import functools

import jax
import jax.numpy as jnp
from jax import lax
from jax.experimental import pallas as pl
from jax.experimental.pallas import tpu as pltpu
from jax.sharding import PartitionSpec as P


EPS = 1e-06
F32 = jnp.float32
BF16 = jnp.bfloat16

COVER = 1 << 31


def call(kernel, outs, *args, scratch=(), flops=1000000, limit=8):
    single = not isinstance(outs, (list, tuple))
    spec = pl.BlockSpec(memory_space=pltpu.VMEM)
    return pl.pallas_call(
        kernel,
        out_shape=outs,
        in_specs=[spec] * len(args),
        out_specs=spec if single else [spec] * len(outs),
        scratch_shapes=list(scratch),
        compiler_params=pltpu.CompilerParams(vmem_limit_bytes=limit << 20),
        cost_estimate=pl.CostEstimate(flops=flops, bytes_accessed=1 << 20, transcendentals=0),
    )(*args)


def shape(dims, dtype):
    return jax.ShapeDtypeStruct(tuple(dims), dtype)


class Layout:
    def __init__(self, batch, tp, dp):
        self.batch, self.tp, self.dp = batch, tp, dp
        self.rows = batch // dp
        self.half = batch // 2
        self.per_tp = batch // tp
        self.chunks = self.per_tp // self.rows

    def side(self, owner, z):
        return pl.multiple_of((owner ^ z) * self.rows, self.rows)

    def place(self, chunk, z, core):
        side = jnp.where(lax.rem(chunk, 2) == core, 0, self.half)
        return pl.multiple_of(side + ((chunk // 2) ^ z) * self.rows, self.rows)


def mesh_place():
    core = lax.rem(lax.axis_index("dp"), 2)
    return lax.axis_index("tp"), lax.axis_index("dp") // 2, core


def partner_exchange(value, axis, masks):
    count = lax.axis_size(axis)
    got = []
    for m in masks:
        got.append(lax.ppermute(value, axis, [(i, i ^ m) for i in range(count)]))
    return got


ORDERS = {
    "sum0": ((3, 1, 2), (3, 1, 2)),
    "sum1": ((2, 3, 1), (2, 3, 1)),
    "out0": ((3, 2, 1), (2, 3, 1)),
    "last": ((3, 2, 1), (3, 2, 1)),
}


def orders(name, count):
    if name in ORDERS and len(ORDERS[name][0]) == count - 1:
        return ORDERS[name]
    return (tuple(range(1, count)),) * 2


def core_exchange(values, axis, name):
    tp, dp = lax.axis_size("tp"), lax.axis_size("dp")
    got = []
    for k, masks in enumerate(zip(*orders(name, tp if axis == "tp" else dp // 2))):
        pairs = []
        for t in range(tp):
            for d in range(dp):
                m = masks[d % 2]
                to = (t ^ m, d) if axis == "tp" else (t, d ^ (2 * m))
                pairs.append((t * dp + d, to[0] * dp + to[1]))
        got.append(lax.ppermute(values[k % len(values)], ("tp", "dp"), pairs))
    return got


def doubling(value, axis, masks):
    stack = value[None]
    for mask in masks:
        (got,) = partner_exchange(stack, axis, [mask])
        if mask == masks[-1]:
            return [stack, got]
        stack = call(join_kernel, shape((2 * stack.shape[0],) + stack.shape[1:], stack.dtype), stack, got)


def join_kernel(first_ref, second_ref, out_ref):
    half = first_ref.shape[0]
    out_ref[:half] = first_ref[...]
    out_ref[half:] = second_ref[...]


def entry(stacks, m):
    size = stacks[0].shape[0]
    return stacks[m // size][m % size]


def as_column(row):
    n = row.shape[1]
    eye = lax.broadcasted_iota(jnp.int32, (n, n), 0) == lax.broadcasted_iota(jnp.int32, (n, n), 1)
    return jnp.sum(jnp.where(eye, jnp.broadcast_to(row, (n, n)), 0), axis=1, keepdims=True)


def length_kernel(lengths_ref, out_ref):
    out_ref[...] = jnp.broadcast_to(as_column(lengths_ref[...]), out_ref.shape)


def state_kernel(lengths_ref, taps_ref, conv_ref, rec_ref, out_ref, low_ref):
    live = lengths_ref[:, 0:1]
    depth = conv_ref.shape[1]
    for layer in range(conv_ref.shape[0]):
        old = jnp.zeros(rec_ref.shape[1:], F32)
        for back in range(1, depth + 1):
            tap = taps_ref[layer, depth - back : depth - back + 1, :].astype(F32)
            old = old + tap * jnp.where(back < live, conv_ref[layer, depth - back].astype(F32), 0.0)
        out_ref[layer, 0] = old
        out_ref[layer, 1] = jnp.where(live > 1, rec_ref[layer], 0.0)
    low_ref[...] = out_ref[...].astype(BF16)


LANES = 128
GROUP = 8


def packed_rows(rows, width):
    return 2 * (width // LANES) * rows + GROUP


def pack(ref, value, gate, square):
    rows, width = value.shape
    count = width // LANES
    for k, block in enumerate((value, gate)):
        for b in range(count):
            start = (k * count + b) * rows
            ref[start : start + rows, :] = block[:, b * LANES : (b + 1) * LANES].astype(ref.dtype)
    high = square.astype(BF16).astype(F32)
    low = square - high
    lane = lax.broadcasted_iota(jnp.int32, (GROUP, LANES), 1)
    tile = jnp.zeros((GROUP, LANES), F32)
    for g in range(rows // GROUP):
        part = slice(g * GROUP, (g + 1) * GROUP)
        tile = jnp.where(lane == g, high[part], jnp.where(lane == g + LANES // 2, low[part], tile))
    ref[2 * count * rows : 2 * count * rows + GROUP, :] = tile.astype(ref.dtype)


def unpack(total, rows, width):
    count = width // LANES
    blocks = [total[b * rows : (b + 1) * rows] for b in range(2 * count)]
    value = jnp.concatenate(blocks[:count], axis=1)
    gate = jnp.concatenate(blocks[count:], axis=1)
    tile = total[2 * count * rows :]
    half = LANES // 2
    square = jnp.concatenate(
        [tile[:, g : g + 1] + tile[:, g + half : g + half + 1] for g in range(rows // GROUP)], axis=0
    )
    return value, gate, square


def by_owner(part, mask, zs, size):
    return jnp.concatenate([part[(m ^ mask) * size : ((m ^ mask) + 1) * size] for m in range(zs)], axis=0)


def to_blocks(ref, start, rows):
    count = rows.shape[0]
    for b in range(rows.shape[1] // LANES):
        ref[start + b * count : start + (b + 1) * count, :] = rows[:, b * LANES : (b + 1) * LANES].astype(ref.dtype)


def from_blocks(ref, start, rows, width):
    return jnp.concatenate(
        [ref[start + b * rows : start + (b + 1) * rows, :] for b in range(width // LANES)], axis=1
    )


def first_kernel(lay, low_ref, high_ref, gain_ref, wi_ref, wg_ref, x_ref, keep_ref, send_ref):
    me, z, core = mesh_place()
    for mask in range(lay.tp):
        owner = me ^ mask
        rows = entry((low_ref, high_ref), mask).astype(F32)
        for i in range(lay.chunks):
            start = lay.place(owner * lay.chunks + i, z, core)
            x_ref[pl.ds(start, lay.rows), :] = rows[i * lay.rows : (i + 1) * lay.rows]
    x = x_ref[...]
    half, tall = lay.half, keep_ref.shape[0]
    square = jnp.sum(x * x, axis=1, keepdims=True)
    scaled = (x * gain_ref[0:1, :]).astype(BF16)
    value = jnp.dot(scaled, wi_ref[0], preferred_element_type=F32)
    gate = jnp.dot(scaled, wg_ref[0], preferred_element_type=F32)
    pack(keep_ref, value[:half], gate[:half], square[:half])
    pack(send_ref, value[half:], gate[half:], square[half:])
    to_blocks(send_ref, tall, x[half:])


def next_kernel(lay, layer, x_old_ref, got_ref, *refs):
    parts, refs = refs[: lay.tp], refs[lay.tp :]
    gain_ref, wi_ref, wg_ref, gain2_ref, wi2_ref, wg2_ref, x_ref, out_ref = refs
    half, depth = lay.half, x_old_ref.shape[1]
    start = got_ref.shape[0] - half * depth // LANES
    total = parts[0][...].astype(F32)
    for part in parts[1:]:
        total = total + part[...].astype(F32)
    x = (x_old_ref[:half] + total[:, :depth]).astype(BF16).astype(F32)
    y = (from_blocks(got_ref, start, half, depth).astype(F32) + total[:, depth:]).astype(BF16).astype(F32)
    x_ref[:, :depth] = x
    x_ref[:, depth:] = y
    square = jnp.sum(x * x, axis=1, keepdims=True) + jnp.sum(y * y, axis=1, keepdims=True)
    scaled = (x * gain_ref[layer : layer + 1, :]).astype(BF16)
    scaled2 = (y * gain2_ref[layer : layer + 1, :]).astype(BF16)

    def both(w, w2):
        return jnp.dot(scaled, w[layer], preferred_element_type=F32) + jnp.dot(
            scaled2, w2[layer], preferred_element_type=F32
        )

    pack(out_ref, both(wi_ref, wi2_ref), both(wg_ref, wg2_ref), square)


def sigmoid(x):
    return 0.5 * jnp.tanh(0.5 * x) + 0.5


def one_minus_square(decay, log_decay):
    u = 2.0 * log_decay
    series = 1.0 + u * (1.0 / 6.0)
    for k in (5.0, 4.0, 3.0, 2.0):
        series = 1.0 + u * (1.0 / k) * series
    return jnp.where(u > -0.25, -u * series, 1.0 - decay * decay)


def add_kernel(keep_ref, got_ref, out_ref):
    out_ref[...] = (keep_ref[...] + got_ref[: keep_ref.shape[0]].astype(F32)).astype(out_ref.dtype)


def recurrence_kernel(lay, layer, features, *refs):
    zs = lay.dp // 2
    sums, refs = refs[:zs], refs[zs:]
    own_ref, low_ref, high_ref, taps_ref, decay_ref, wr_ref, wj_ref, *extra, out_ref, value_ref, rec_ref = refs
    rows, half, width = lay.rows, lay.half, taps_ref.shape[2]
    states = [own_ref] + [entry((low_ref, high_ref), m) for m in range(1, zs)]
    old = jnp.concatenate([state[layer, 0].astype(F32) for state in states], axis=0)
    previous = jnp.concatenate([state[layer, 1].astype(F32) for state in states], axis=0)
    value_in = gate_in = square = None
    me, z, core = mesh_place()
    south, north = orders(f"sum{layer}", zs)
    for mask in range(zs):
        if mask == 0:
            part = sums[0][...]
        elif south.index(mask) == north.index(mask):
            part = sums[1 + south.index(mask)][...]
        else:
            part = jnp.where(core == 0, sums[1 + south.index(mask)][...], sums[1 + north.index(mask)][...])
        terms = [by_owner(t, mask, zs, rows) for t in unpack(part.astype(F32), half, width)]
        if mask == 0:
            value_in, gate_in, square = terms
        else:
            value_in, gate_in, square = value_in + terms[0], gate_in + terms[1], square + terms[2]
    scale = lax.rsqrt(square / features + EPS)
    value_in = value_in * scale
    gate_in = gate_in * scale
    last = taps_ref.shape[1] - 1
    conv_out = taps_ref[layer, last : last + 1, :].astype(F32) * value_in + old
    conv_low = conv_out.astype(BF16)
    blocks, block = wr_ref.shape[1], wr_ref.shape[2]

    maps = [
        jnp.dot(
            conv_low[:, b * block : (b + 1) * block],
            jnp.concatenate([wr_ref[layer, b], wj_ref[layer, b]], axis=1),
            preferred_element_type=F32,
        )
        for b in range(blocks)
    ]
    rec_gate = sigmoid(jnp.concatenate([m[:, :block] for m in maps], axis=1))
    inp_gate = sigmoid(jnp.concatenate([m[:, block:] for m in maps], axis=1))
    log_decay = -8.0 * rec_gate * jax.nn.softplus(-decay_ref[layer : layer + 1, :])
    decay = jnp.exp(log_decay)
    hidden = decay * previous + jnp.sqrt(one_minus_square(decay, log_decay)) * (inp_gate * conv_out)
    readout = (hidden * jax.nn.gelu(gate_in)).astype(BF16)
    if len(extra) == 2:
        for k, w_ref in enumerate(extra):
            depth = w_ref.shape[2]
            columns = slice(k * depth, (k + 1) * depth)
            out_ref[:, columns] = jnp.dot(readout, w_ref[layer], preferred_element_type=F32).astype(BF16)
    else:
        (x_ref,) = extra
        out_ref[:half] = readout
        me, z, _ = mesh_place()
        depth = x_ref.shape[1] // 2
        for i in range(lay.chunks // 2):
            start = lay.side(me * (lay.chunks // 2) + i, z)
            out_ref[half + i * rows : half + (i + 1) * rows] = x_ref[pl.ds(start, rows), depth:].astype(BF16)
    value_ref[...] = value_in[:rows].astype(BF16)
    rec_ref[...] = hidden[:rows]


def last_output_kernel(lay, layer, own_ref, other_ref, w_ref, x_ref, *refs):
    outs, held = refs[:-1], refs[-1]
    half, rows, depth = lay.half, lay.rows, held.shape[1]
    held[:half] = jnp.dot(own_ref[:half], w_ref[layer], preferred_element_type=F32)
    held[half:] = jnp.dot(other_ref[:half], w_ref[layer], preferred_element_type=F32)
    me, z, core = mesh_place()
    far = other_ref[half:].astype(F32)
    masks = zip(*orders("last", lay.tp))
    masks = [0] + [jnp.where(core == 0, a, b) if a != b else a for a, b in masks]
    for k, (mask, out) in enumerate(zip(masks, outs)):
        for i in range(lay.chunks):
            start = lay.place((me ^ mask) * lay.chunks + i, z, core)
            piece = held[pl.ds(start, rows), :]
            if k == 0:
                near = x_ref[pl.ds(lay.side(me * (lay.chunks // 2) + i // 2, z), rows), :depth]
                piece = piece + jnp.where(core == i % 2, near, far[i // 2 * rows : (i // 2 + 1) * rows])
            out[i * rows : (i + 1) * rows, :] = piece.astype(out.dtype)


def final_kernel(own_ref, *refs):
    parts, out_ref = refs[:-1], refs[-1]
    total = own_ref[...]
    for part in parts:
        total = total + part[...].astype(F32)
    out_ref[...] = total.astype(BF16)


def blocks(
    tokens,
    norm_gain,
    w_input,
    w_gate,
    w_recur,
    w_inject,
    conv_weight,
    decay_param,
    w_output,
    lengths,
    conv_state,
    rec_state,
):
    tp, dp = lax.axis_size("tp"), lax.axis_size("dp")
    lay = Layout(tokens.shape[0] * tp, tp, dp)
    depth, features = tokens.shape[1], tokens.shape[1] * dp
    width = rec_state.shape[2]
    half, batch = lay.half, lay.batch
    layers = w_input.shape[0]

    tall = packed_rows(half, width)
    bits = lambda n: [1 << k for k in range(n.bit_length() - 1)]
    live = call(length_kernel, shape((lay.rows, LANES), jnp.int32), lengths[None, :], flops=COVER)
    state, low = call(
        state_kernel,
        [shape((layers, 2, lay.rows, width), t) for t in (F32, BF16)],
        live,
        conv_weight,
        conv_state,
        rec_state,
    )
    rows = doubling(tokens, "tp", bits(tp))
    states = [state] + doubling(low, "dp", [2 * m for m in bits(dp // 2)])
    sent = half * depth // LANES
    block = [
        shape((half, width), BF16),
        shape((lay.rows, width), BF16),
        shape((lay.rows, width), F32),
    ]
    weights = (norm_gain, w_input, w_gate)
    x, keep, send = call(
        functools.partial(first_kernel, lay),
        [shape((batch, depth), F32), shape((tall, LANES), F32), shape((tall + sent, LANES), BF16)],
        *rows,
        *weights,
    )
    (got,) = partner_exchange(send, "dp", [1])
    summed = call(add_kernel, shape((tall, LANES), BF16), keep, got)
    conv_list, rec_list = [], []
    for layer in range(layers):
        last = layer == layers - 1
        if layer > 0:
            x, summed = call(
                functools.partial(next_kernel, lay, layer),
                [shape((half, 2 * depth), F32), shape((tall, LANES), BF16)],
                *before,
                *parts,
                *weights,
                *weights2,
            )
        sums = [summed] + core_exchange([summed], "z", f"sum{layer}")
        if layer == 0:
            out2, *weights2 = [partner_exchange(w, "dp", [1])[0] for w in (w_output,) + weights]
        block[0] = shape((half + lay.per_tp // 2, width) if last else (half, 2 * depth), BF16)
        readout, value, hidden = call(
            functools.partial(recurrence_kernel, lay, layer, features),
            block,
            *sums,
            *states,
            conv_weight,
            decay_param,
            w_recur,
            w_inject,
            *([x] if last else [w_output, out2]),
        )
        if not last:
            parts = [readout] + core_exchange([readout], "tp", f"out{layer}")
            before = (x, got)
        else:
            (other,) = partner_exchange(readout, "dp", [1])
            own, *pieces = call(
                functools.partial(last_output_kernel, lay, layer),
                [shape((lay.per_tp, depth), F32)] + [shape((lay.per_tp, depth), BF16)] * (tp - 1),
                readout,
                other,
                w_output,
                x,
                scratch=[pltpu.VMEM((batch, depth), F32)],
            )
            parts = [own] + core_exchange(pieces, "tp", "last")
        conv_list.append(jnp.concatenate([conv_state[layer, 1:], value[None]], axis=0))
        rec_list.append(hidden)
    mixed = call(final_kernel, shape((lay.per_tp, depth), BF16), *parts)
    return mixed, jnp.stack(conv_list), jnp.stack(rec_list)


def solution(mesh):
    placed = (
        P("tp", "dp"),
        P(None, "dp"),
        P(None, "dp", "tp"),
        P(None, "dp", "tp"),
        P(None, "tp", None, None),
        P(None, "tp", None, None),
        P(None, None, "tp"),
        P(None, "tp"),
        P(None, "tp", "dp"),
        P("dp"),
        P(None, None, "dp", "tp"),
        P(None, "dp", "tp"),
    )

    return jax.shard_map(
        blocks,
        mesh=mesh,
        in_specs=placed,
        out_specs=(P("tp", "dp"), P(None, None, "dp", "tp"), P(None, "dp", "tp")),
        check_vma=False,
    )
```

```python
import functools

import jax
import jax.numpy as jnp
from jax import lax
from jax.experimental import pallas as pl
from jax.experimental.pallas import tpu as pltpu
from jax.sharding import PartitionSpec as P


EPS = 1e-06
F32 = jnp.float32
BF16 = jnp.bfloat16

COVER = 1 << 31


def call(kernel, outs, *args, scratch=(), flops=1000000, limit=8):
    single = not isinstance(outs, (list, tuple))
    spec = pl.BlockSpec(memory_space=pltpu.VMEM)
    return pl.pallas_call(
        kernel,
        out_shape=outs,
        in_specs=[spec] * len(args),
        out_specs=spec if single else [spec] * len(outs),
        scratch_shapes=list(scratch),
        compiler_params=pltpu.CompilerParams(vmem_limit_bytes=limit << 20),
        cost_estimate=pl.CostEstimate(flops=flops, bytes_accessed=1 << 20, transcendentals=0),
    )(*args)


def shape(dims, dtype):
    return jax.ShapeDtypeStruct(tuple(dims), dtype)


class Layout:
    def __init__(self, batch, tp, dp):
        self.batch, self.tp, self.dp = batch, tp, dp
        self.rows = batch // dp
        self.half = batch // 2
        self.per_tp = batch // tp
        self.chunks = self.per_tp // self.rows

    def side(self, owner, z):
        return pl.multiple_of((owner ^ z) * self.rows, self.rows)

    def place(self, chunk, z, core):
        side = jnp.where(lax.rem(chunk, 2) == core, 0, self.half)
        return pl.multiple_of(side + ((chunk // 2) ^ z) * self.rows, self.rows)


def mesh_place():
    core = lax.rem(lax.axis_index("dp"), 2)
    return lax.axis_index("tp"), lax.axis_index("dp") // 2, core


def partner_exchange(value, axis, masks):
    count = lax.axis_size(axis)
    got = []
    for m in masks:
        got.append(lax.ppermute(value, axis, [(i, i ^ m) for i in range(count)]))
    return got


ORDERS = {
    "sum0": ((3, 1, 2), (3, 1, 2)),
    "sum1": ((2, 3, 1), (2, 3, 1)),
    "out0": ((3, 2, 1), (2, 3, 1)),
    "last": ((3, 2, 1), (3, 2, 1)),
}


def orders(name, count):
    if name in ORDERS and len(ORDERS[name][0]) == count - 1:
        return ORDERS[name]
    return (tuple(range(1, count)),) * 2


def core_exchange(values, axis, name):
    tp, dp = lax.axis_size("tp"), lax.axis_size("dp")
    got = []
    for k, masks in enumerate(zip(*orders(name, tp if axis == "tp" else dp // 2))):
        pairs = []
        for t in range(tp):
            for d in range(dp):
                m = masks[d % 2]
                to = (t ^ m, d) if axis == "tp" else (t, d ^ (2 * m))
                pairs.append((t * dp + d, to[0] * dp + to[1]))
        got.append(lax.ppermute(values[k % len(values)], ("tp", "dp"), pairs))
    return got


def doubling(value, axis, masks):
    stack = value[None]
    for mask in masks:
        (got,) = partner_exchange(stack, axis, [mask])
        if mask == masks[-1]:
            return [stack, got]
        stack = call(join_kernel, shape((2 * stack.shape[0],) + stack.shape[1:], stack.dtype), stack, got)


def join_kernel(first_ref, second_ref, out_ref):
    half = first_ref.shape[0]
    out_ref[:half] = first_ref[...]
    out_ref[half:] = second_ref[...]


def entry(stacks, m):
    size = stacks[0].shape[0]
    return stacks[m // size][m % size]


def as_column(row):
    n = row.shape[1]
    eye = lax.broadcasted_iota(jnp.int32, (n, n), 0) == lax.broadcasted_iota(jnp.int32, (n, n), 1)
    return jnp.sum(jnp.where(eye, jnp.broadcast_to(row, (n, n)), 0), axis=1, keepdims=True)


def length_kernel(lengths_ref, out_ref):
    out_ref[...] = jnp.broadcast_to(as_column(lengths_ref[...]), out_ref.shape)


def state_kernel(lengths_ref, taps_ref, conv_ref, rec_ref, out_ref, low_ref):
    live = lengths_ref[:, 0:1]
    depth = conv_ref.shape[1]
    for layer in range(conv_ref.shape[0]):
        old = jnp.zeros(rec_ref.shape[1:], F32)
        for back in range(1, depth + 1):
            tap = taps_ref[layer, depth - back : depth - back + 1, :].astype(F32)
            old = old + tap * jnp.where(back < live, conv_ref[layer, depth - back].astype(F32), 0.0)
        out_ref[layer, 0] = old
        out_ref[layer, 1] = jnp.where(live > 1, rec_ref[layer], 0.0)
    low_ref[...] = out_ref[...].astype(BF16)


LANES = 128
GROUP = 8


def packed_rows(rows, width):
    return 2 * (width // LANES) * rows + GROUP


def pack(ref, value, gate, square):
    rows, width = value.shape
    count = width // LANES
    for k, block in enumerate((value, gate)):
        for b in range(count):
            start = (k * count + b) * rows
            ref[start : start + rows, :] = block[:, b * LANES : (b + 1) * LANES].astype(ref.dtype)
    high = square.astype(BF16).astype(F32)
    low = square - high
    lane = lax.broadcasted_iota(jnp.int32, (GROUP, LANES), 1)
    tile = jnp.zeros((GROUP, LANES), F32)
    for g in range(rows // GROUP):
        part = slice(g * GROUP, (g + 1) * GROUP)
        tile = jnp.where(lane == g, high[part], jnp.where(lane == g + LANES // 2, low[part], tile))
    ref[2 * count * rows : 2 * count * rows + GROUP, :] = tile.astype(ref.dtype)


def unpack(total, rows, width):
    count = width // LANES
    blocks = [total[b * rows : (b + 1) * rows] for b in range(2 * count)]
    value = jnp.concatenate(blocks[:count], axis=1)
    gate = jnp.concatenate(blocks[count:], axis=1)
    tile = total[2 * count * rows :]
    half = LANES // 2
    square = jnp.concatenate(
        [tile[:, g : g + 1] + tile[:, g + half : g + half + 1] for g in range(rows // GROUP)], axis=0
    )
    return value, gate, square


def by_owner(part, mask, zs, size):
    return jnp.concatenate([part[(m ^ mask) * size : ((m ^ mask) + 1) * size] for m in range(zs)], axis=0)


def to_blocks(ref, start, rows):
    count = rows.shape[0]
    for b in range(rows.shape[1] // LANES):
        ref[start + b * count : start + (b + 1) * count, :] = rows[:, b * LANES : (b + 1) * LANES].astype(ref.dtype)


def from_blocks(ref, start, rows, width):
    return jnp.concatenate(
        [ref[start + b * rows : start + (b + 1) * rows, :] for b in range(width // LANES)], axis=1
    )


def first_kernel(lay, low_ref, high_ref, gain_ref, wi_ref, wg_ref, x_ref, keep_ref, send_ref):
    me, z, core = mesh_place()
    for mask in range(lay.tp):
        owner = me ^ mask
        rows = entry((low_ref, high_ref), mask).astype(F32)
        for i in range(lay.chunks):
            start = lay.place(owner * lay.chunks + i, z, core)
            x_ref[pl.ds(start, lay.rows), :] = rows[i * lay.rows : (i + 1) * lay.rows]
    x = x_ref[...]
    half, tall = lay.half, keep_ref.shape[0]
    square = jnp.sum(x * x, axis=1, keepdims=True)
    scaled = (x * gain_ref[0:1, :]).astype(BF16)
    value = jnp.dot(scaled, wi_ref[0], preferred_element_type=F32)
    gate = jnp.dot(scaled, wg_ref[0], preferred_element_type=F32)
    pack(keep_ref, value[:half], gate[:half], square[:half])
    pack(send_ref, value[half:], gate[half:], square[half:])
    to_blocks(send_ref, tall, x[half:])


def next_kernel(lay, layer, x_old_ref, got_ref, *refs):
    parts, refs = refs[: lay.tp], refs[lay.tp :]
    gain_ref, wi_ref, wg_ref, gain2_ref, wi2_ref, wg2_ref, x_ref, out_ref = refs
    half, depth = lay.half, x_old_ref.shape[1]
    start = got_ref.shape[0] - half * depth // LANES
    total = parts[0][...].astype(F32)
    for part in parts[1:]:
        total = total + part[...].astype(F32)
    x = (x_old_ref[:half] + total[:, :depth]).astype(BF16).astype(F32)
    y = (from_blocks(got_ref, start, half, depth).astype(F32) + total[:, depth:]).astype(BF16).astype(F32)
    x_ref[:, :depth] = x
    x_ref[:, depth:] = y
    square = jnp.sum(x * x, axis=1, keepdims=True) + jnp.sum(y * y, axis=1, keepdims=True)
    scaled = (x * gain_ref[layer : layer + 1, :]).astype(BF16)
    scaled2 = (y * gain2_ref[layer : layer + 1, :]).astype(BF16)

    def both(w, w2):
        return jnp.dot(scaled, w[layer], preferred_element_type=F32) + jnp.dot(
            scaled2, w2[layer], preferred_element_type=F32
        )

    pack(out_ref, both(wi_ref, wi2_ref), both(wg_ref, wg2_ref), square)


def one_minus_square(decay, log_decay):
    u = 2.0 * log_decay
    series = 1.0 + u * (1.0 / 6.0)
    for k in (5.0, 4.0, 3.0, 2.0):
        series = 1.0 + u * (1.0 / k) * series
    return jnp.where(u > -0.25, -u * series, 1.0 - decay * decay)


def add_kernel(keep_ref, got_ref, out_ref):
    out_ref[...] = (keep_ref[...] + got_ref[: keep_ref.shape[0]].astype(F32)).astype(out_ref.dtype)


def recurrence_kernel(lay, layer, features, *refs):
    zs = lay.dp // 2
    sums, refs = refs[:zs], refs[zs:]
    own_ref, low_ref, high_ref, taps_ref, decay_ref, wr_ref, wj_ref, *extra, out_ref, value_ref, rec_ref = refs
    rows, half, width = lay.rows, lay.half, taps_ref.shape[2]
    states = [own_ref] + [entry((low_ref, high_ref), m) for m in range(1, zs)]
    old = jnp.concatenate([state[layer, 0].astype(F32) for state in states], axis=0)
    previous = jnp.concatenate([state[layer, 1].astype(F32) for state in states], axis=0)
    value_in = gate_in = square = None
    me, z, core = mesh_place()
    south, north = orders(f"sum{layer}", zs)
    for mask in range(zs):
        if mask == 0:
            part = sums[0][...]
        elif south.index(mask) == north.index(mask):
            part = sums[1 + south.index(mask)][...]
        else:
            part = jnp.where(core == 0, sums[1 + south.index(mask)][...], sums[1 + north.index(mask)][...])
        terms = [by_owner(t, mask, zs, rows) for t in unpack(part.astype(F32), half, width)]
        if mask == 0:
            value_in, gate_in, square = terms
        else:
            value_in, gate_in, square = value_in + terms[0], gate_in + terms[1], square + terms[2]
    scale = lax.rsqrt(square / features + EPS)
    value_in = value_in * scale
    gate_in = gate_in * scale
    last = taps_ref.shape[1] - 1
    conv_out = taps_ref[layer, last : last + 1, :].astype(F32) * value_in + old
    conv_low = conv_out.astype(BF16)
    blocks, block = wr_ref.shape[1], wr_ref.shape[2]

    maps = [
        jnp.dot(
            conv_low[:, b * block : (b + 1) * block],
            jnp.concatenate([wr_ref[layer, b], wj_ref[layer, b]], axis=1),
            preferred_element_type=F32,
        )
        for b in range(blocks)
    ]
    rec_gate = jax.nn.sigmoid(jnp.concatenate([m[:, :block] for m in maps], axis=1))
    inp_gate = jax.nn.sigmoid(jnp.concatenate([m[:, block:] for m in maps], axis=1))
    log_decay = -8.0 * rec_gate * jax.nn.softplus(-decay_ref[layer : layer + 1, :])
    decay = jnp.exp(log_decay)
    hidden = decay * previous + jnp.sqrt(one_minus_square(decay, log_decay)) * (inp_gate * conv_out)
    readout = (hidden * jax.nn.gelu(gate_in)).astype(BF16)
    if len(extra) == 2:
        for k, w_ref in enumerate(extra):
            depth = w_ref.shape[2]
            columns = slice(k * depth, (k + 1) * depth)
            out_ref[:, columns] = jnp.dot(readout, w_ref[layer], preferred_element_type=F32).astype(BF16)
    else:
        (x_ref,) = extra
        out_ref[:half] = readout
        me, z, _ = mesh_place()
        depth = x_ref.shape[1] // 2
        for i in range(lay.chunks // 2):
            start = lay.side(me * (lay.chunks // 2) + i, z)
            out_ref[half + i * rows : half + (i + 1) * rows] = x_ref[pl.ds(start, rows), depth:].astype(BF16)
    value_ref[...] = value_in[:rows].astype(BF16)
    rec_ref[...] = hidden[:rows]


def last_output_kernel(lay, layer, own_ref, other_ref, w_ref, x_ref, *refs):
    outs, held = refs[:-1], refs[-1]
    half, rows, depth = lay.half, lay.rows, held.shape[1]
    held[:half] = jnp.dot(own_ref[:half], w_ref[layer], preferred_element_type=F32)
    held[half:] = jnp.dot(other_ref[:half], w_ref[layer], preferred_element_type=F32)
    me, z, core = mesh_place()
    far = other_ref[half:].astype(F32)
    masks = zip(*orders("last", lay.tp))
    masks = [0] + [jnp.where(core == 0, a, b) if a != b else a for a, b in masks]
    for k, (mask, out) in enumerate(zip(masks, outs)):
        for i in range(lay.chunks):
            start = lay.place((me ^ mask) * lay.chunks + i, z, core)
            piece = held[pl.ds(start, rows), :]
            if k == 0:
                near = x_ref[pl.ds(lay.side(me * (lay.chunks // 2) + i // 2, z), rows), :depth]
                piece = piece + jnp.where(core == i % 2, near, far[i // 2 * rows : (i // 2 + 1) * rows])
            out[i * rows : (i + 1) * rows, :] = piece.astype(out.dtype)


def final_kernel(own_ref, *refs):
    parts, out_ref = refs[:-1], refs[-1]
    total = own_ref[...]
    for part in parts:
        total = total + part[...].astype(F32)
    out_ref[...] = total.astype(BF16)


def blocks(
    tokens,
    norm_gain,
    w_input,
    w_gate,
    w_recur,
    w_inject,
    conv_weight,
    decay_param,
    w_output,
    lengths,
    conv_state,
    rec_state,
):
    tp, dp = lax.axis_size("tp"), lax.axis_size("dp")
    lay = Layout(tokens.shape[0] * tp, tp, dp)
    depth, features = tokens.shape[1], tokens.shape[1] * dp
    width = rec_state.shape[2]
    half, batch = lay.half, lay.batch
    layers = w_input.shape[0]

    tall = packed_rows(half, width)
    bits = lambda n: [1 << k for k in range(n.bit_length() - 1)]
    live = call(length_kernel, shape((lay.rows, LANES), jnp.int32), lengths[None, :], flops=COVER)
    state, low = call(
        state_kernel,
        [shape((layers, 2, lay.rows, width), t) for t in (F32, BF16)],
        live,
        conv_weight,
        conv_state,
        rec_state,
    )
    rows = doubling(tokens, "tp", bits(tp))
    states = [state] + doubling(low, "dp", [2 * m for m in bits(dp // 2)])
    sent = half * depth // LANES
    block = [
        shape((half, width), BF16),
        shape((lay.rows, width), BF16),
        shape((lay.rows, width), F32),
    ]
    weights = (norm_gain, w_input, w_gate)
    x, keep, send = call(
        functools.partial(first_kernel, lay),
        [shape((batch, depth), F32), shape((tall, LANES), F32), shape((tall + sent, LANES), BF16)],
        *rows,
        *weights,
    )
    (got,) = partner_exchange(send, "dp", [1])
    summed = call(add_kernel, shape((tall, LANES), BF16), keep, got)
    conv_list, rec_list = [], []
    for layer in range(layers):
        last = layer == layers - 1
        if layer > 0:
            x, summed = call(
                functools.partial(next_kernel, lay, layer),
                [shape((half, 2 * depth), F32), shape((tall, LANES), BF16)],
                *before,
                *parts,
                *weights,
                *weights2,
            )
        sums = [summed] + core_exchange([summed], "z", f"sum{layer}")
        if layer == 0:
            out2, *weights2 = [partner_exchange(w, "dp", [1])[0] for w in (w_output,) + weights]
        block[0] = shape((half + lay.per_tp // 2, width) if last else (half, 2 * depth), BF16)
        readout, value, hidden = call(
            functools.partial(recurrence_kernel, lay, layer, features),
            block,
            *sums,
            *states,
            conv_weight,
            decay_param,
            w_recur,
            w_inject,
            *([x] if last else [w_output, out2]),
        )
        if not last:
            parts = [readout] + core_exchange([readout], "tp", f"out{layer}")
            before = (x, got)
        else:
            (other,) = partner_exchange(readout, "dp", [1])
            own, *pieces = call(
                functools.partial(last_output_kernel, lay, layer),
                [shape((lay.per_tp, depth), F32)] + [shape((lay.per_tp, depth), BF16)] * (tp - 1),
                readout,
                other,
                w_output,
                x,
                scratch=[pltpu.VMEM((batch, depth), F32)],
            )
            parts = [own] + core_exchange(pieces, "tp", "last")
        conv_list.append(jnp.concatenate([conv_state[layer, 1:], value[None]], axis=0))
        rec_list.append(hidden)
    mixed = call(final_kernel, shape((lay.per_tp, depth), BF16), *parts)
    return mixed, jnp.stack(conv_list), jnp.stack(rec_list)


def solution(mesh):
    placed = (
        P("tp", "dp"),
        P(None, "dp"),
        P(None, "dp", "tp"),
        P(None, "dp", "tp"),
        P(None, "tp", None, None),
        P(None, "tp", None, None),
        P(None, None, "tp"),
        P(None, "tp"),
        P(None, "tp", "dp"),
        P("dp"),
        P(None, None, "dp", "tp"),
        P(None, "dp", "tp"),
    )

    return jax.shard_map(
        blocks,
        mesh=mesh,
        in_specs=placed,
        out_specs=(P("tp", "dp"), P(None, None, "dp", "tp"), P(None, "dp", "tp")),
        check_vma=False,
    )
```

```python
import functools

import jax
import jax.numpy as jnp
from jax import lax
from jax.experimental import pallas as pl
from jax.experimental.pallas import tpu as pltpu
from jax.sharding import PartitionSpec as P


EPS = 1e-06
F32 = jnp.float32
BF16 = jnp.bfloat16

COVER = 1 << 31


def call(kernel, outs, *args, scratch=(), flops=1000000, limit=8):
    single = not isinstance(outs, (list, tuple))
    spec = pl.BlockSpec(memory_space=pltpu.VMEM)
    return pl.pallas_call(
        kernel,
        out_shape=outs,
        in_specs=[spec] * len(args),
        out_specs=spec if single else [spec] * len(outs),
        scratch_shapes=list(scratch),
        compiler_params=pltpu.CompilerParams(vmem_limit_bytes=limit << 20),
        cost_estimate=pl.CostEstimate(flops=flops, bytes_accessed=1 << 20, transcendentals=0),
    )(*args)


def shape(dims, dtype):
    return jax.ShapeDtypeStruct(tuple(dims), dtype)


class Layout:
    def __init__(self, batch, tp, dp):
        self.batch, self.tp, self.dp = batch, tp, dp
        self.rows = batch // dp
        self.half = batch // 2
        self.per_tp = batch // tp
        self.chunks = self.per_tp // self.rows

    def side(self, owner, z):
        return pl.multiple_of((owner ^ z) * self.rows, self.rows)

    def place(self, chunk, z, core):
        side = jnp.where(lax.rem(chunk, 2) == core, 0, self.half)
        return pl.multiple_of(side + ((chunk // 2) ^ z) * self.rows, self.rows)


def mesh_place():
    core = lax.rem(lax.axis_index("dp"), 2)
    return lax.axis_index("tp"), lax.axis_index("dp") // 2, core


def partner_exchange(value, axis, masks):
    count = lax.axis_size(axis)
    got = []
    for m in masks:
        got.append(lax.ppermute(value, axis, [(i, i ^ m) for i in range(count)]))
    return got


ORDERS = {
    "sum0": ((3, 1, 2), (3, 1, 2)),
    "sum1": ((2, 3, 1), (2, 3, 1)),
    "out0": ((3, 2, 1), (2, 3, 1)),
    "last": ((3, 2, 1), (3, 2, 1)),
}


def orders(name, count):
    if name in ORDERS and len(ORDERS[name][0]) == count - 1:
        return ORDERS[name]
    return (tuple(range(1, count)),) * 2


def core_exchange(values, axis, name):
    tp, dp = lax.axis_size("tp"), lax.axis_size("dp")
    got = []
    for k, masks in enumerate(zip(*orders(name, tp if axis == "tp" else dp // 2))):
        pairs = []
        for t in range(tp):
            for d in range(dp):
                m = masks[d % 2]
                to = (t ^ m, d) if axis == "tp" else (t, d ^ (2 * m))
                pairs.append((t * dp + d, to[0] * dp + to[1]))
        got.append(lax.ppermute(values[k % len(values)], ("tp", "dp"), pairs))
    return got


def doubling(value, axis, masks):
    stack = value[None]
    for mask in masks:
        (got,) = partner_exchange(stack, axis, [mask])
        if mask == masks[-1]:
            return [stack, got]
        stack = call(join_kernel, shape((2 * stack.shape[0],) + stack.shape[1:], stack.dtype), stack, got)


def join_kernel(first_ref, second_ref, out_ref):
    half = first_ref.shape[0]
    out_ref[:half] = first_ref[...]
    out_ref[half:] = second_ref[...]


def entry(stacks, m):
    size = stacks[0].shape[0]
    return stacks[m // size][m % size]


def as_column(row):
    n = row.shape[1]
    eye = lax.broadcasted_iota(jnp.int32, (n, n), 0) == lax.broadcasted_iota(jnp.int32, (n, n), 1)
    return jnp.sum(jnp.where(eye, jnp.broadcast_to(row, (n, n)), 0), axis=1, keepdims=True)


def length_kernel(lengths_ref, out_ref):
    out_ref[...] = jnp.broadcast_to(as_column(lengths_ref[...]), out_ref.shape)


def state_kernel(lengths_ref, taps_ref, conv_ref, rec_ref, out_ref, low_ref):
    live = lengths_ref[:, 0:1]
    depth = conv_ref.shape[1]
    for layer in range(conv_ref.shape[0]):
        old = jnp.zeros(rec_ref.shape[1:], F32)
        for back in range(1, depth + 1):
            tap = taps_ref[layer, depth - back : depth - back + 1, :].astype(F32)
            old = old + tap * jnp.where(back < live, conv_ref[layer, depth - back].astype(F32), 0.0)
        out_ref[layer, 0] = old
        out_ref[layer, 1] = jnp.where(live > 1, rec_ref[layer], 0.0)
    low_ref[...] = out_ref[...].astype(BF16)


LANES = 128
GROUP = 8


def packed_rows(rows, width):
    return 2 * (width // LANES) * rows + GROUP


def pack(ref, value, gate, square):
    rows, width = value.shape
    count = width // LANES
    for k, block in enumerate((value, gate)):
        for b in range(count):
            start = (k * count + b) * rows
            ref[start : start + rows, :] = block[:, b * LANES : (b + 1) * LANES].astype(ref.dtype)
    high = square.astype(BF16).astype(F32)
    low = square - high
    lane = lax.broadcasted_iota(jnp.int32, (GROUP, LANES), 1)
    tile = jnp.zeros((GROUP, LANES), F32)
    for g in range(rows // GROUP):
        part = slice(g * GROUP, (g + 1) * GROUP)
        tile = jnp.where(lane == g, high[part], jnp.where(lane == g + LANES // 2, low[part], tile))
    ref[2 * count * rows : 2 * count * rows + GROUP, :] = tile.astype(ref.dtype)


def unpack(total, rows, width):
    count = width // LANES
    blocks = [total[b * rows : (b + 1) * rows] for b in range(2 * count)]
    value = jnp.concatenate(blocks[:count], axis=1)
    gate = jnp.concatenate(blocks[count:], axis=1)
    tile = total[2 * count * rows :]
    half = LANES // 2
    square = jnp.concatenate(
        [tile[:, g : g + 1] + tile[:, g + half : g + half + 1] for g in range(rows // GROUP)], axis=0
    )
    return value, gate, square


def by_owner(part, mask, zs, size):
    return jnp.concatenate([part[(m ^ mask) * size : ((m ^ mask) + 1) * size] for m in range(zs)], axis=0)


def to_blocks(ref, start, rows):
    count = rows.shape[0]
    for b in range(rows.shape[1] // LANES):
        ref[start + b * count : start + (b + 1) * count, :] = rows[:, b * LANES : (b + 1) * LANES].astype(ref.dtype)


def from_blocks(ref, start, rows, width):
    return jnp.concatenate(
        [ref[start + b * rows : start + (b + 1) * rows, :] for b in range(width // LANES)], axis=1
    )


def first_kernel(lay, low_ref, high_ref, gain_ref, wi_ref, wg_ref, x_ref, keep_ref, send_ref):
    me, z, core = mesh_place()
    for mask in range(lay.tp):
        owner = me ^ mask
        rows = entry((low_ref, high_ref), mask).astype(F32)
        for i in range(lay.chunks):
            start = lay.place(owner * lay.chunks + i, z, core)
            x_ref[pl.ds(start, lay.rows), :] = rows[i * lay.rows : (i + 1) * lay.rows]
    x = x_ref[...]
    half, tall = lay.half, keep_ref.shape[0]
    square = jnp.sum(x * x, axis=1, keepdims=True)
    scaled = (x * gain_ref[0:1, :]).astype(BF16)
    value = jnp.dot(scaled, wi_ref[0], preferred_element_type=F32)
    gate = jnp.dot(scaled, wg_ref[0], preferred_element_type=F32)
    pack(keep_ref, value[:half], gate[:half], square[:half])
    pack(send_ref, value[half:], gate[half:], square[half:])
    to_blocks(send_ref, tall, x[half:])


def next_kernel(lay, layer, x_old_ref, got_ref, *refs):
    parts, refs = refs[: lay.tp], refs[lay.tp :]
    gain_ref, wi_ref, wg_ref, gain2_ref, wi2_ref, wg2_ref, x_ref, out_ref = refs
    half, depth = lay.half, x_old_ref.shape[1]
    start = got_ref.shape[0] - half * depth // LANES
    total = parts[0][...].astype(F32)
    for part in parts[1:]:
        total = total + part[...].astype(F32)
    x = (x_old_ref[:half] + total[:, :depth]).astype(BF16).astype(F32)
    y = (from_blocks(got_ref, start, half, depth).astype(F32) + total[:, depth:]).astype(BF16).astype(F32)
    x_ref[:, :depth] = x
    x_ref[:, depth:] = y
    square = jnp.sum(x * x, axis=1, keepdims=True) + jnp.sum(y * y, axis=1, keepdims=True)
    scaled = (x * gain_ref[layer : layer + 1, :]).astype(BF16)
    scaled2 = (y * gain2_ref[layer : layer + 1, :]).astype(BF16)

    def both(w, w2):
        return jnp.dot(scaled, w[layer], preferred_element_type=F32) + jnp.dot(
            scaled2, w2[layer - 1], preferred_element_type=F32
        )

    pack(out_ref, both(wi_ref, wi2_ref), both(wg_ref, wg2_ref), square)


def one_minus_square(decay, log_decay):
    u = 2.0 * log_decay
    series = 1.0 + u * (1.0 / 6.0)
    for k in (5.0, 4.0, 3.0, 2.0):
        series = 1.0 + u * (1.0 / k) * series
    return jnp.where(u > -0.25, -u * series, 1.0 - decay * decay)


def add_kernel(keep_ref, got_ref, out_ref):
    out_ref[...] = (keep_ref[...] + got_ref[: keep_ref.shape[0]].astype(F32)).astype(out_ref.dtype)


def recurrence_kernel(lay, layer, features, *refs):
    zs = lay.dp // 2
    sums, refs = refs[:zs], refs[zs:]
    own_ref, low_ref, high_ref, taps_ref, decay_ref, wr_ref, wj_ref, *extra, out_ref, value_ref, rec_ref = refs
    rows, half, width = lay.rows, lay.half, taps_ref.shape[2]
    states = [own_ref] + [entry((low_ref, high_ref), m) for m in range(1, zs)]
    old = jnp.concatenate([state[layer, 0].astype(F32) for state in states], axis=0)
    previous = jnp.concatenate([state[layer, 1].astype(F32) for state in states], axis=0)
    value_in = gate_in = square = None
    me, z, core = mesh_place()
    south, north = orders(f"sum{layer}", zs)
    for mask in range(zs):
        if mask == 0:
            part = sums[0][...]
        elif south.index(mask) == north.index(mask):
            part = sums[1 + south.index(mask)][...]
        else:
            part = jnp.where(core == 0, sums[1 + south.index(mask)][...], sums[1 + north.index(mask)][...])
        terms = [by_owner(t, mask, zs, rows) for t in unpack(part.astype(F32), half, width)]
        if mask == 0:
            value_in, gate_in, square = terms
        else:
            value_in, gate_in, square = value_in + terms[0], gate_in + terms[1], square + terms[2]
    scale = lax.rsqrt(square / features + EPS)
    value_in = value_in * scale
    gate_in = gate_in * scale
    last = taps_ref.shape[1] - 1
    conv_out = taps_ref[layer, last : last + 1, :].astype(F32) * value_in + old
    conv_low = conv_out.astype(BF16)
    blocks, block = wr_ref.shape[1], wr_ref.shape[2]

    maps = [
        jnp.dot(
            conv_low[:, b * block : (b + 1) * block],
            jnp.concatenate([wr_ref[layer, b], wj_ref[layer, b]], axis=1),
            preferred_element_type=F32,
        )
        for b in range(blocks)
    ]
    rec_gate = jax.nn.sigmoid(jnp.concatenate([m[:, :block] for m in maps], axis=1))
    inp_gate = jax.nn.sigmoid(jnp.concatenate([m[:, block:] for m in maps], axis=1))
    log_decay = -8.0 * rec_gate * jax.nn.softplus(-decay_ref[layer : layer + 1, :])
    decay = jnp.exp(log_decay)
    hidden = decay * previous + jnp.sqrt(one_minus_square(decay, log_decay)) * (inp_gate * conv_out)
    readout = (hidden * jax.nn.gelu(gate_in)).astype(BF16)
    if len(extra) == 2:
        for k, w_ref in enumerate(extra):
            depth = w_ref.shape[2]
            columns = slice(k * depth, (k + 1) * depth)
            out_ref[:, columns] = jnp.dot(readout, w_ref[layer], preferred_element_type=F32).astype(BF16)
    else:
        (x_ref,) = extra
        out_ref[:half] = readout
        me, z, _ = mesh_place()
        depth = x_ref.shape[1] // 2
        for i in range(lay.chunks // 2):
            start = lay.side(me * (lay.chunks // 2) + i, z)
            out_ref[half + i * rows : half + (i + 1) * rows] = x_ref[pl.ds(start, rows), depth:].astype(BF16)
    value_ref[...] = value_in[:rows].astype(BF16)
    rec_ref[...] = hidden[:rows]


def last_output_kernel(lay, layer, own_ref, other_ref, w_ref, x_ref, *refs):
    outs, held = refs[:-1], refs[-1]
    half, rows, depth = lay.half, lay.rows, held.shape[1]
    held[:half] = jnp.dot(own_ref[:half], w_ref[layer], preferred_element_type=F32)
    held[half:] = jnp.dot(other_ref[:half], w_ref[layer], preferred_element_type=F32)
    me, z, core = mesh_place()
    far = other_ref[half:].astype(F32)
    masks = zip(*orders("last", lay.tp))
    masks = [0] + [jnp.where(core == 0, a, b) if a != b else a for a, b in masks]
    for k, (mask, out) in enumerate(zip(masks, outs)):
        for i in range(lay.chunks):
            start = lay.place((me ^ mask) * lay.chunks + i, z, core)
            piece = held[pl.ds(start, rows), :]
            if k == 0:
                near = x_ref[pl.ds(lay.side(me * (lay.chunks // 2) + i // 2, z), rows), :depth]
                piece = piece + jnp.where(core == i % 2, near, far[i // 2 * rows : (i // 2 + 1) * rows])
            out[i * rows : (i + 1) * rows, :] = piece.astype(out.dtype)


def final_kernel(own_ref, *refs):
    parts, out_ref = refs[:-1], refs[-1]
    total = own_ref[...]
    for part in parts:
        total = total + part[...].astype(F32)
    out_ref[...] = total.astype(BF16)


def blocks(
    tokens,
    norm_gain,
    w_input,
    w_gate,
    w_recur,
    w_inject,
    conv_weight,
    decay_param,
    w_output,
    lengths,
    conv_state,
    rec_state,
):
    tp, dp = lax.axis_size("tp"), lax.axis_size("dp")
    lay = Layout(tokens.shape[0] * tp, tp, dp)
    depth, features = tokens.shape[1], tokens.shape[1] * dp
    width = rec_state.shape[2]
    half, batch = lay.half, lay.batch
    layers = w_input.shape[0]

    tall = packed_rows(half, width)
    bits = lambda n: [1 << k for k in range(n.bit_length() - 1)]
    live = call(length_kernel, shape((lay.rows, LANES), jnp.int32), lengths[None, :], flops=COVER)
    state, low = call(
        state_kernel,
        [shape((layers, 2, lay.rows, width), t) for t in (F32, BF16)],
        live,
        conv_weight,
        conv_state,
        rec_state,
    )
    rows = doubling(tokens, "tp", bits(tp))
    states = [state] + doubling(low, "dp", [2 * m for m in bits(dp // 2)])
    sent = half * depth // LANES
    block = [
        shape((half, width), BF16),
        shape((lay.rows, width), BF16),
        shape((lay.rows, width), F32),
    ]
    weights = (norm_gain, w_input, w_gate)
    x, keep, send = call(
        functools.partial(first_kernel, lay),
        [shape((batch, depth), F32), shape((tall, LANES), F32), shape((tall + sent, LANES), BF16)],
        *rows,
        *weights,
    )
    (got,) = partner_exchange(send, "dp", [1])
    summed = call(add_kernel, shape((tall, LANES), BF16), keep, got)
    conv_list, rec_list = [], []
    for layer in range(layers):
        last = layer == layers - 1
        if layer > 0:
            x, summed = call(
                functools.partial(next_kernel, lay, layer),
                [shape((half, 2 * depth), F32), shape((tall, LANES), BF16)],
                *before,
                *parts,
                *weights,
                *weights2,
            )
        sums = [summed] + core_exchange([summed], "z", f"sum{layer}")
        if layer == 0:
            out2, *weights2 = [
                partner_exchange(w, "dp", [1])[0] for w in (w_output[:-1], norm_gain, w_input[1:], w_gate[1:])
            ]
        block[0] = shape((half + lay.per_tp // 2, width) if last else (half, 2 * depth), BF16)
        readout, value, hidden = call(
            functools.partial(recurrence_kernel, lay, layer, features),
            block,
            *sums,
            *states,
            conv_weight,
            decay_param,
            w_recur,
            w_inject,
            *([x] if last else [w_output, out2]),
        )
        if not last:
            parts = [readout] + core_exchange([readout], "tp", f"out{layer}")
            before = (x, got)
        else:
            (other,) = partner_exchange(readout, "dp", [1])
            own, *pieces = call(
                functools.partial(last_output_kernel, lay, layer),
                [shape((lay.per_tp, depth), F32)] + [shape((lay.per_tp, depth), BF16)] * (tp - 1),
                readout,
                other,
                w_output,
                x,
                scratch=[pltpu.VMEM((batch, depth), F32)],
            )
            parts = [own] + core_exchange(pieces, "tp", "last")
        conv_list.append(jnp.concatenate([conv_state[layer, 1:], value[None]], axis=0))
        rec_list.append(hidden)
    mixed = call(final_kernel, shape((lay.per_tp, depth), BF16), *parts)
    return mixed, jnp.stack(conv_list), jnp.stack(rec_list)


def solution(mesh):
    placed = (
        P("tp", "dp"),
        P(None, "dp"),
        P(None, "dp", "tp"),
        P(None, "dp", "tp"),
        P(None, "tp", None, None),
        P(None, "tp", None, None),
        P(None, None, "tp"),
        P(None, "tp"),
        P(None, "tp", "dp"),
        P("dp"),
        P(None, None, "dp", "tp"),
        P(None, "dp", "tp"),
    )

    return jax.shard_map(
        blocks,
        mesh=mesh,
        in_specs=placed,
        out_specs=(P("tp", "dp"), P(None, None, "dp", "tp"), P(None, "dp", "tp")),
        check_vma=False,
    )
```
